32 devices in a mesh: kv: 8 (over z, y), tp: 4 (over x, core).
Axes of the slice: x: 2, y: 2, z: 4, core: 2. Of those that a mesh axis runs over, the one named last changes fastest.
Arguments:
- tokens: bfloat16 [256, 4, 2048], P(None, None, ('kv', 'tp')), may hold values from -520 to 520
- input_norm_gain: bfloat16 [2048], replicated, may hold values from 0.099609375 to 1.8984375
- query_weight: bfloat16 [2048, 2048], P(None, 'kv'), may hold values from -0.125 to 0.125
- key_weight: bfloat16 [2048, 2048], P(None, 'kv'), may hold values from -0.125 to 0.125
- value_weight: bfloat16 [2048, 16, 128], P(None, 'kv', 'tp'), may hold values from -1.14904852 to 1.14904852
- output_gate_weight: bfloat16 [2048, 16, 128], P(None, 'kv', 'tp'), may hold values from -0.125 to 0.125
- strength_weight: bfloat16 [2048, 16], P(None, 'kv'), may hold values from -0.125 to 0.125
- decay_weight: bfloat16 [2048, 16], P(None, 'kv'), may hold values from -0.125 to 0.125
- head_decay_rate: float32 [16], P('kv'), may hold values from 0.005 to 1.5
- proposal_log_decay: float32 [256, 4, 16], P(None, None, 'kv'), may hold values from -0.69 to 0
- head_norm_gain: bfloat16 [128], P('tp'), may hold values from 0.099609375 to 1.8984375
- output_weight: bfloat16 [16, 128, 2048], P('kv', 'tp'), may hold values from -1.14904852 to 1.14904852
- output_norm_gain: bfloat16 [2048], P(('kv', 'tp')), may hold values from 0.099609375 to 1.8984375
- state: float32 [256, 16, 128, 128], P(None, 'kv', 'tp'), may hold values from -4.5961941 to 4.5961941
- previous_keys: bfloat16 [256, 4, 2048], P(None, None, 'kv'), may hold values from -6 to 6
- previous_values: bfloat16 [256, 4, 16, 128], P(None, None, 'kv', 'tp'), may hold values from -52 to 52
- previous_log_decay: float32 [256, 4, 16], P(None, None, 'kv'), may hold values from -0.7 to -0.02
- previous_strengths: float32 [256, 4, 16], P(None, None, 'kv'), may hold values from 0.1 to 0.9
- accepted: int32 [256], replicated, may hold values from 0 to 4
- parent: int32 [256, 4], replicated, may hold values from -1 to 2, as said below
Outputs:
- layer_out: bfloat16 [256, 4, 2048], P(None, None, ('kv', 'tp'))
- accepted_state: float32 [256, 16, 128, 128], P(None, 'kv', 'tp')
The draws below stay inside these ranges and needn't reach their ends.
Inputs may be any that keep to these rules, and one draw needn't show every extreme that they name: parent[b, i] is -1 or a proposal index below i; -1 means that proposal i follows the accepted old proposals directly.
All inputs are finite; a program needn't handle non-finite values.
Results may differ from the reference program's by a relative error of at most 0.019.
Values may be sent and summed in bfloat16 or wider, within the bound.
A program may use at most 128 MiB of HBM per device.

```python
import jax
import jax.numpy as jnp
from jax import lax

D = 2048
H = 16
HD = 128
PROP = 4
SEQS = 256


def column_scales(key, count):
    position = jnp.arange(count, dtype=jnp.float32) / max(count - 1, 1)
    spread = jax.random.uniform(key, (count,), jnp.float32)
    return jnp.exp(jnp.log(3.0) * position + jnp.log(3.4) * spread)


def rough_base(key, shape):
    base = jax.random.normal(key, shape, jnp.float32)
    return jnp.clip(base, -5.0, 5.0)


def draw_tokens(key, part):
    subkeys = jax.random.split(jax.random.fold_in(key, 11), 3)
    base = rough_base(subkeys[0], (SEQS, PROP, D))
    rowscale = jnp.exp(jnp.log(10.0) * jax.random.uniform(subkeys[2], (SEQS, PROP, 1), jnp.float32))
    return (base * column_scales(subkeys[1], D)[None, None, :] * rowscale).astype(jnp.bfloat16)


def draw_output_weight(key, part):
    subkeys = jax.random.split(jax.random.fold_in(key, 23), 2)
    base = jax.random.normal(subkeys[0], (H, HD, D), jnp.float32)
    base = jnp.clip(base, -5.0, 5.0)
    scaled = base * (H * HD) ** (-0.5) * column_scales(subkeys[1], D)[None, None, :]
    return scaled.astype(jnp.bfloat16)


def draw_value_weight(key, part):
    subkeys = jax.random.split(jax.random.fold_in(key, 61), 2)
    base = rough_base(subkeys[0], (D, H, HD))
    return (base * D ** (-0.5) * column_scales(subkeys[1], HD)[None, None, :]).astype(jnp.bfloat16)


def draw_state(key, part):
    subkeys = jax.random.split(jax.random.fold_in(key, 67), 2)
    base = rough_base(subkeys[0], (SEQS, H, HD, HD))
    return base * HD ** (-0.5) * column_scales(subkeys[1], HD)[None, None, :, None]


def draw_previous_values(key, part):
    subkeys = jax.random.split(jax.random.fold_in(key, 71), 2)
    base = rough_base(subkeys[0], (SEQS, PROP, H, HD))
    return (base * column_scales(subkeys[1], HD)[None, None, None, :]).astype(jnp.bfloat16)


def draw_head_decay_rate(key, part):
    uniform_part = jax.random.uniform(jax.random.fold_in(key, 31), (H,), jnp.float32)
    lowest = 0.02
    highest = 1.5
    return jnp.exp(jnp.log(lowest) + uniform_part * (jnp.log(highest) - jnp.log(lowest)))


def draw_proposal_log_decay(key, part):
    subkeys = jax.random.split(jax.random.fold_in(key, 41), 2)
    chosen = (jax.random.randint(subkeys[0], (SEQS, PROP, H), 0, 4) == 0).astype(jnp.float32)
    depth = jax.random.uniform(subkeys[1], (SEQS, PROP, H), jnp.float32, 0.22, 0.69)
    return -depth * chosen


def draw_parent(key, part):
    raw_bits = jax.random.randint(jax.random.fold_in(key, 53), (SEQS, PROP), 0, 1 << 20)
    column = jnp.arange(PROP, dtype=jnp.int32)
    return (raw_bits % (column[None, :] + 1) - 1).astype(jnp.int32)


def set_ends(drawn, rng, low, top_value):
    extent = drawn.shape
    spot = [jax.random.randint(jax.random.fold_in(rng, axis), (), 0, extent[axis]) for axis in range(len(extent))]
    drawn = drawn.at[tuple(spot)].set(low)
    longest = extent.index(max(extent))
    spot[longest] = (spot[longest] + 1) % extent[longest]
    return drawn.at[tuple(spot)].set(top_value)


def levels(own_key, shape, shards, smallest, high):
    gain, own = 1.0, jax.random.fold_in(own_key, 6)
    for dim, parts in shards:
        draws = jnp.exp(jax.random.uniform(jax.random.fold_in(own, dim), (parts,), jnp.float32, smallest / len(shards), high / len(shards)))
        gain = gain * jnp.repeat(draws, shape[dim] // parts).reshape([-1 if axis == dim else 1 for axis in range(len(shape))])
    return gain


def normal_values(own_key, extent, scale, most, cuts=(), kind=jnp.bfloat16):
    values = scale * jax.random.normal(own_key, extent, jnp.float32)
    if cuts:
        values = values * levels(own_key, extent, cuts, -0.22, 0.18)
    return jnp.clip(values, -most, most).astype(kind)


def setup_inputs(seed: int = 0) -> dict:
    key_list = jax.random.split(jax.random.key(seed), 21)
    tokens = draw_tokens(jax.random.fold_in(key_list[20], 71), 0)
    input_norm_gain = jnp.clip(1.0 + 0.18 * jax.random.normal(key_list[1], (D,), jnp.float32), 0.099609375, 1.8984375).astype(jnp.bfloat16)
    query_weight = normal_values(key_list[2], (D, H * HD), D ** -0.5, 0.125, ((1, 8),))
    key_weight = normal_values(key_list[3], (D, H * HD), D ** -0.5, 0.125, ((1, 8),))
    value_weight = draw_value_weight(jax.random.fold_in(key_list[20], 71), 0)
    output_gate_weight = normal_values(key_list[5], (D, H, HD), D ** -0.5, 0.125, ((1, 8), (2, 4)))
    strength_weight = normal_values(key_list[6], (D, H), D ** -0.5, 0.125, ((1, 8),))
    decay_weight = normal_values(key_list[7], (D, H), D ** -0.5, 0.125, ((1, 8),))
    head_decay_rate = draw_head_decay_rate(jax.random.fold_in(key_list[20], 71), 0)
    proposal_log_decay = draw_proposal_log_decay(jax.random.fold_in(key_list[20], 71), 0)
    head_norm_gain = jnp.clip(1.0 + 0.18 * jax.random.normal(key_list[10], (HD,), jnp.float32), 0.099609375, 1.8984375).astype(jnp.bfloat16)
    output_weight = draw_output_weight(jax.random.fold_in(key_list[20], 71), 0)
    output_norm_gain = jnp.clip(1.0 + 0.18 * jax.random.normal(key_list[12], (D,), jnp.float32), 0.099609375, 1.8984375).astype(jnp.bfloat16)
    state = draw_state(jax.random.fold_in(key_list[20], 71), 0)
    previous_keys = normal_values(key_list[14], (SEQS, PROP, H * HD), 1.0, 6.0, ((2, 8),))
    previous_values = draw_previous_values(jax.random.fold_in(key_list[20], 71), 0)
    previous_log_decay = jnp.clip(-0.7 + 0.68 * jax.random.uniform(key_list[16], (SEQS, PROP, H), jnp.float32) ** levels(key_list[16], (SEQS, PROP, H), ((2, 8),), -0.2, 0.2), -0.7, -0.02)
    previous_strengths = jnp.clip(0.1 + 0.79999997 * jax.random.uniform(key_list[17], (SEQS, PROP, H), jnp.float32) ** levels(key_list[17], (SEQS, PROP, H), ((2, 8),), -0.2, 0.2), 0.1, 0.9)
    accepted = set_ends(jax.random.randint(key_list[18], (SEQS,), 0, PROP + 1), jax.random.fold_in(key_list[18], 1), 0, PROP).astype(jnp.int32)
    parent = draw_parent(jax.random.fold_in(key_list[20], 71), 0)
    return {"tokens": tokens, "input_norm_gain": input_norm_gain, "query_weight": query_weight, "key_weight": key_weight, "value_weight": value_weight, "output_gate_weight": output_gate_weight, "strength_weight": strength_weight, "decay_weight": decay_weight, "head_decay_rate": head_decay_rate, "proposal_log_decay": proposal_log_decay, "head_norm_gain": head_norm_gain, "output_weight": output_weight, "output_norm_gain": output_norm_gain, "state": state, "previous_keys": previous_keys, "previous_values": previous_values, "previous_log_decay": previous_log_decay, "previous_strengths": previous_strengths, "accepted": accepted, "parent": parent}


epsilon = 1e-06

def unit_rows(matrix):
    return matrix * lax.rsqrt(lax.optimization_barrier(jnp.sum(matrix * matrix, axis=-1, keepdims=True)) + epsilon)

def exact_product(form, left, right):
    return jnp.einsum(form, left, right, precision=lax.Precision.HIGHEST)

def visibility(parent):
    sequence_count, proposal_count = parent.shape
    position = jnp.arange(proposal_count, dtype=jnp.int32)
    parent_hot = (parent[:, :, None] == position[None, None, :]).astype(jnp.float32)
    ancestry = []
    for row_index in range(proposal_count):
        ancestor_row = parent_hot[:, row_index, :]
        if row_index > 0:
            earlier = jnp.stack(ancestry, axis=1)
            ancestor_row = ancestor_row + exact_product('bj,bjk->bk', parent_hot[:, row_index, :row_index], earlier)
        ancestry.append(ancestor_row)
    ancestor = jnp.stack(ancestry, axis=1)
    chain = (position[:, None] > position[None, :]).astype(jnp.float32)
    upper = jnp.concatenate([jnp.broadcast_to(chain, (sequence_count, proposal_count, proposal_count)), jnp.zeros((sequence_count, proposal_count, proposal_count), jnp.float32)], axis=2)
    lower = jnp.concatenate([jnp.ones((sequence_count, proposal_count, proposal_count), jnp.float32), ancestor], axis=2)
    return jnp.concatenate([upper, lower], axis=1)

def split_heads(matrix, sequence_count, proposal_count, number_of_heads):
    return matrix.astype(jnp.float32).reshape(sequence_count, proposal_count, number_of_heads, -1).transpose(0, 2, 1, 3)

def delta_recursion(query_projected, key_projected, value_projected, output_gate_logits, write_strength_logits, decay_logits, decay_speed, proposal_group, head_norm_gain, state, previous_keys, previous_values, previous_log_decay, previous_strengths, accepted, parent, channel_count_total):
    sequence_count, number_of_heads, value_dim, head_dim = state.shape
    proposal_count = parent.shape[1]
    queries = unit_rows(split_heads(query_projected, sequence_count, proposal_count, number_of_heads)) * head_dim ** (-0.5)
    new_keys = unit_rows(split_heads(key_projected, sequence_count, proposal_count, number_of_heads))
    old_keys = unit_rows(split_heads(previous_keys, sequence_count, proposal_count, number_of_heads))
    new_values = split_heads(value_projected, sequence_count, proposal_count, number_of_heads)
    old_values = split_heads(previous_values, sequence_count, proposal_count, number_of_heads)
    zgate = split_heads(output_gate_logits, sequence_count, proposal_count, number_of_heads)
    beta_new = jax.nn.sigmoid(write_strength_logits.reshape(sequence_count, proposal_count, number_of_heads)).transpose(0, 2, 1)
    fresh_decay = (-decay_speed[None, None, :] * jax.nn.softplus(decay_logits.reshape(sequence_count, proposal_count, number_of_heads)) + proposal_group).transpose(0, 2, 1)
    position = jnp.arange(proposal_count, dtype=jnp.int32)
    live = (position[None, :] < accepted[:, None]).astype(jnp.float32)[:, None, :]
    beta_old = previous_strengths.transpose(0, 2, 1) * live
    decay_old = previous_log_decay.transpose(0, 2, 1) * live
    keys_all = jnp.concatenate([old_keys, new_keys], axis=2)
    values_all = jnp.concatenate([old_values, new_values], axis=2)
    beta_all = jnp.concatenate([beta_old, beta_new], axis=2)
    decay_all = jnp.concatenate([decay_old, fresh_decay], axis=2)
    visible = visibility(parent)
    gamma_sum = decay_all + exact_product('bij,bhj->bhi', visible, decay_all)
    gamma_diff = gamma_sum[:, :, :, None] - gamma_sum[:, :, None, :]
    decay_pair = jnp.exp(jnp.minimum(gamma_diff, 0.0)) * visible[:, None]
    coupling = beta_all[..., None] * exact_product('bhid,bhjd->bhij', keys_all, keys_all) * decay_pair
    right_side = jnp.concatenate([beta_all[..., None] * values_all, (beta_all * jnp.exp(gamma_sum))[..., None] * keys_all], axis=-1)
    solved = []
    for row_index in range(2 * proposal_count):
        current = right_side[:, :, row_index]
        if row_index > 0:
            current = current - exact_product('bhj,bhjd->bhd', coupling[:, :, row_index, :row_index], jnp.stack(solved, axis=2))
        solved.append(current)
    solution = jnp.stack(solved, axis=2)
    update = solution[..., :value_dim] - exact_product('bhcd,bhed->bhce', solution[..., value_dim:], state)
    identity = jnp.eye(2 * proposal_count, dtype=jnp.float32)
    seen = visible[:, proposal_count:] + identity[proposal_count:][None]
    reach = jnp.exp(jnp.minimum(gamma_diff[:, :, proposal_count:], 0.0)) * seen[:, None]
    query_key = exact_product('bhid,bhjd->bhij', queries, keys_all) * reach
    readout = exact_product('bhid,bhed->bhie', queries * jnp.exp(gamma_sum[:, :, proposal_count:])[..., None], state)
    readout = readout + exact_product('bhij,bhje->bhie', query_key, update)
    squares = channel_count_total(lax.optimization_barrier(jnp.sum(readout * readout, axis=-1)))
    readout = readout * lax.rsqrt(squares / head_dim + epsilon)[..., None]
    readout = readout * head_norm_gain.astype(jnp.float32) * jax.nn.silu(zgate)
    blended_rows = readout.transpose(0, 2, 1, 3).reshape(sequence_count * proposal_count, number_of_heads * value_dim)
    blended_rows = blended_rows.astype(jnp.bfloat16)
    last_gamma = gamma_sum[:, :, proposal_count - 1:proposal_count]
    key_weighted = old_keys * jnp.exp(last_gamma - gamma_sum[:, :, :proposal_count])[..., None]
    accepted_state = jnp.exp(last_gamma)[..., None] * state + exact_product('bhcd,bhce->bhed', key_weighted, update[:, :, :proposal_count])
    return (blended_rows, accepted_state)

def kept_channel_total(squares):
    return squares

def reference(tokens, input_norm_gain, query_weight, key_weight, value_weight, output_gate_weight, strength_weight, decay_weight, head_decay_rate, proposal_log_decay, head_norm_gain, output_weight, output_norm_gain, state, previous_keys, previous_values, previous_log_decay, previous_strengths, accepted, parent):
    sequence_count, proposal_count, width = tokens.shape
    features = tokens.astype(jnp.float32)
    normed = features * lax.rsqrt(lax.optimization_barrier(jnp.mean(features * features, axis=-1, keepdims=True)) + epsilon)
    normed = (normed * input_norm_gain.astype(jnp.float32)).astype(jnp.bfloat16)
    flat_rows = normed.reshape(sequence_count * proposal_count, width)
    query_projected = jnp.dot(flat_rows, query_weight, preferred_element_type=jnp.float32).astype(jnp.bfloat16)
    key_projected = jnp.dot(flat_rows, key_weight, preferred_element_type=jnp.float32).astype(jnp.bfloat16)
    value_projected = jnp.dot(flat_rows, value_weight.reshape(width, -1), preferred_element_type=jnp.float32).astype(jnp.bfloat16)
    output_gate_logits = jnp.dot(flat_rows, output_gate_weight.reshape(width, -1), preferred_element_type=jnp.float32).astype(jnp.bfloat16)
    write_strength_logits = jnp.dot(flat_rows, strength_weight, preferred_element_type=jnp.float32)
    decay_logits = jnp.dot(flat_rows, decay_weight, preferred_element_type=jnp.float32)
    blended_rows, accepted_state = delta_recursion(query_projected, key_projected, value_projected, output_gate_logits, write_strength_logits, decay_logits, head_decay_rate, proposal_log_decay, head_norm_gain, state, previous_keys, previous_values, previous_log_decay, previous_strengths, accepted, parent, kept_channel_total)
    combined = jnp.dot(blended_rows, output_weight.reshape(-1, width), preferred_element_type=jnp.float32)
    combined = combined * lax.rsqrt(lax.optimization_barrier(jnp.mean(combined * combined, axis=-1, keepdims=True)) + epsilon)
    layer_out = (combined * output_norm_gain.astype(jnp.float32)).astype(jnp.bfloat16).reshape(sequence_count, proposal_count, width)
    return (layer_out, accepted_state)
```

```python
import functools

import jax
import jax.numpy as jnp
from jax import lax
from jax.experimental import pallas as pl
from jax.experimental.pallas import tpu as pltpu
from jax.sharding import PartitionSpec as P

epsilon = 1e-06
GROUP = 16
AXES = ("kv", "tp")
MESH = pl.DeviceIdType.MESH
f32, bf16 = jnp.float32, jnp.bfloat16


class Grid:
    def __init__(self, kv, tp):
        self.kv, self.tp = kv, tp
        self.x = tp // 2
        self.y = self.x if kv % self.x == 0 else 1
        self.z = kv // self.y
        self.sizes = (self.z, self.y, self.x)

    def here(self):
        kv, tp = lax.axis_index("kv"), lax.axis_index("tp")
        self.at = (kv // self.y, lax.rem(kv, self.y), tp // 2)
        self.core = lax.rem(tp, 2)

    def shift(self, offset):
        return tuple(lax.rem(a + o % n, n) for a, o, n in zip(self.at, offset, self.sizes))

    def device(self, offset, flip=0):
        z, y, x = self.shift(offset)
        core = 1 - self.core if flip else self.core
        return (z * self.y + y, x * 2 + core)

    def chip(self, offset):
        z, y, x = self.shift(offset)
        return (z * self.y + y) * self.x + x

    def group(self, offset):
        z, y, _ = self.shift(offset)
        return z * self.y + y


def offsets(sizes):
    return [(a, b, c) for a in range(sizes[0]) for b in range(sizes[1]) for c in range(sizes[2])]


def negated(offset, sizes):
    return tuple(-o % n for o, n in zip(offset, sizes))


def meet(grid, peers):
    peers = set(peers) | {(negated(o, grid.sizes), f) for o, f in peers}
    peers = sorted(peers - {((0, 0, 0), 0)})
    barrier = pltpu.get_barrier_semaphore()
    for offset, flip in peers:
        pl.semaphore_signal(
            barrier, inc=1, device_id=grid.device(offset, flip), device_id_type=MESH
        )
    pl.semaphore_wait(barrier, len(peers))


def remote(src, dst, send, recv, device):
    return pltpu.make_async_remote_copy(
        src_ref=src, dst_ref=dst, send_sem=send, recv_sem=recv, device_id=device,
        device_id_type=MESH,
    )


def tree(sizes, order):
    first, second, third = order
    steps = []
    for offset in offsets(sizes):
        onward = []
        if offset[second] == 0 and offset[third] == 0 and offset[first] < sizes[first] - 1:
            onward.append(first)
        if offset[third] == 0 and offset[second] < sizes[second] - 1:
            onward.append(second)
        if offset[third] < sizes[third] - 1:
            onward.append(third)
        steps.append((offset, onward))
    return steps


def unit(dim, sign):
    return tuple(sign if d == dim else 0 for d in range(3))


def plan(sizes, orders, pieces, stagger):
    events = []
    for p in range(pieces):
        for half, (order, sign) in enumerate(orders):
            for offset, onward in tree(sizes, order):
                events.append((sum(offset) + stagger * p, p, half, offset, onward))
    return sorted(events, key=lambda e: (e[0], e[1], e[3], e[2]))


class Spread:
    def __init__(self, grid, sizes, orders, pieces, stagger, place, halves, send, recv, both):
        self.grid, self.sizes, self.orders, self.pieces = grid, sizes, orders, pieces
        self.place, self.halves = place, halves
        self.send, self.recv, self.both = send, recv, both
        self.events = plan(sizes, orders, pieces, stagger)

    def slot(self, offset):
        a, b, c = offset
        return (a * self.sizes[1] + b) * self.sizes[2] + c

    def source(self, half, offset):
        sign = self.orders[half][1]
        return tuple(-sign * o for o in offset)

    def view(self, p, half, offset):
        return self.place(p, half, self.source(half, offset), self.grid.core)

    def copy(self, p, half, offset, dim):
        sign = self.orders[half][1]
        landed = tuple(o + (1 if d == dim else 0) for d, o in enumerate(offset))
        here = self.view(p, half, offset)
        return remote(
            here, here, self.send.at[p], self.recv.at[p, half, self.slot(landed)],
            self.grid.device(unit(dim, sign)),
        )

    def share(self, p, half, offset):
        here = self.view(p, half, offset)
        return remote(
            here, here, self.both.at[0, p], self.both.at[1, p], self.grid.device((0, 0, 0), 1)
        )

    def run(self, finish):
        left = [0] * self.pieces
        for _, p, half, offset, onward in self.events:
            left[p] += 1
        for _, p, half, offset, onward in self.events:
            if any(offset):
                here = self.view(p, half, offset)
                remote(
                    here, here, self.send.at[p], self.recv.at[p, half, self.slot(offset)],
                    self.grid.device((0, 0, 0), 1),
                ).wait_recv()
                for dim in onward:
                    self.copy(p, half, offset, dim).start()
                self.share(p, half, offset).start()
            left[p] -= 1
            if left[p] == 0:
                finish(p)

    def begin(self, p):
        for _, q, half, offset, onward in self.events:
            if q == p and not any(offset):
                for dim in onward:
                    self.copy(p, half, offset, dim).start()
                self.share(p, half, offset).start()

    def shared(self, p, whole):
        remote(whole, whole, self.both.at[0, p], self.both.at[1, p],
               self.grid.device((0, 0, 0), 1)).wait_recv()

    def sent(self, p, whole, rest):
        far = self.grid.device((0, 0, 0), 1)
        remote(rest, rest, self.send.at[p], self.both.at[1, p], far).wait_send()
        remote(whole, whole, self.both.at[0, p], self.both.at[1, p], far).wait_send()


ORDERS = (((0, 1, 2), 1), ((0, 2, 1), -1))
FLAT = (((0, 1, 2), 1), ((0, 1, 2), -1))
STAGGER = 2


def project_kernel(
    kv, tp,
    tok, gain, wq, wk, wv, wz, ws, wd, rate, extra, old_strength, old_decay, accepted, parent, wo,
    q_out, k_out, v_out, z_out, sc_out, wx_out,
    xt, wt, gcol, wqk, wout, wx, local, send, recv, both, wsend, wrecv,
):
    grid = Grid(kv, tp)
    grid.here()
    pieces, own, seqs = tok.shape
    width = gain.shape[1]
    cols = wq.shape[1]
    small = wv.shape[0]
    heads = rate.shape[1]
    hd = cols // heads
    part = wout.shape[1] // kv
    half_width = seqs // 2

    def place(p, half, offset, core):
        return xt.at[p, grid.chip(offset), core, :, pl.ds(half * half_width, half_width)]

    loads = [
        pltpu.make_async_copy(tok, xt.at[:, grid.chip((0, 0, 0)), grid.core], local.at[0]),
        pltpu.make_async_copy(wo, wout, local.at[1]),
        pltpu.make_async_copy(wq, wqk.at[0], local.at[2]),
        pltpu.make_async_copy(wk, wqk.at[1], local.at[3]),
        pltpu.make_async_copy(wv, wt.at[pl.ds(2 * cols, small)], local.at[4]),
        pltpu.make_async_copy(wz, wt.at[pl.ds(2 * cols + small, small)], local.at[5]),
    ]
    for load in loads:
        load.start()

    plane = [o for o in offsets((grid.z, grid.y, 1)) if any(o)]
    peers = [(unit(d, s), 0) for d in range(3) for s in (1, -1) if grid.sizes[d] > 1]
    peers = [(tuple(o % n for o, n in zip(off, grid.sizes)), f) for off, f in peers]
    peers += [(o, 0) for o in plane] + [((0, 0, 0), 1)]
    meet(grid, peers)

    spread = Spread(
        grid, grid.sizes, ORDERS, pieces, STAGGER, place, 2, send, recv, both
    )
    loads[0].wait()
    for p in range(pieces):
        spread.begin(p)
    loads[1].wait()
    mine = grid.group((0, 0, 0))
    for index, offset in enumerate(plane):
        start = pl.multiple_of(grid.group(offset) * part, part)
        remote(
            wout.at[:, pl.ds(start, part)], wx.at[mine, grid.core],
            wsend.at[0], wrecv.at[index], grid.device(offset),
        ).start()
    wx[mine, grid.core] = wout[:, pl.ds(pl.multiple_of(mine * part, part), part)]

    for first in range(0, width, 128):
        piece = gain[:, first : first + 128].astype(f32)
        gcol[first : first + 128, :] = jnp.broadcast_to(piece, (128, 128)).T
    loads[2].wait()
    loads[3].wait()
    for which in range(2):
        for first in range(0, width, 256):
            piece = wqk[which, first : first + 256, :].astype(f32)
            wt[which * cols : (which + 1) * cols, first : first + 256] = piece.T.astype(bf16)
    loads[4].wait()
    loads[5].wait()
    tail = wt.shape[0] - 2 * cols - 2 * small
    rows = [ws[...].astype(f32), wd[...].astype(f32)]
    rows.append(jnp.zeros((tail - 2 * heads, width), f32))
    wt[2 * cols + 2 * small :, :] = jnp.concatenate(rows, axis=0).astype(bf16)

    chips = kv * tp // 2

    def finish(p):
        spread.shared(p, xt.at[p, :, 1 - grid.core])
        x = xt[p].reshape(width, seqs).astype(f32)
        square = jnp.sum(x * x, axis=0, keepdims=True)
        scale = lax.rsqrt(square / width + epsilon)
        g = jnp.concatenate([gcol[...]] * (seqs // 128), axis=1)
        normed = (x * scale * g).astype(bf16)
        out = jnp.dot(wt[...], normed, preferred_element_type=f32)
        for index, ref in enumerate((q_out, k_out)):
            ref[p] = out[index * cols : (index + 1) * cols].T.astype(bf16)
        v_out[p] = out[2 * cols : 2 * cols + small].astype(bf16)
        z_out[p] = out[2 * cols + small : 2 * cols + 2 * small].astype(bf16)
        side = out[2 * cols + 2 * small :]
        live = jnp.where(accepted[...] > p, 1.0, 0.0)
        for h in range(heads):
            strength = side[h : h + 1]
            decay = side[heads + h : heads + h + 1]
            beta = 1.0 / (1.0 + jnp.exp(-strength))
            soft = jnp.maximum(decay, 0.0) + jnp.log1p(jnp.exp(-jnp.abs(decay)))
            g_new = -rate[0:1, h : h + 1] * soft + extra[p, h : h + 1, :]
            zero = jnp.zeros((1, seqs), f32)
            sc_out[p, h] = jnp.concatenate(
                [
                    old_strength[p, h : h + 1, :] * live,
                    old_decay[p, h : h + 1, :] * live,
                    beta,
                    g_new,
                    parent[p : p + 1, :].astype(f32),
                    zero, zero, zero,
                ],
                axis=0,
            )

    spread.run(finish)

    for index, offset in enumerate(plane):
        origin = grid.group(negated(offset, grid.sizes))
        here = wx.at[origin, grid.core]
        remote(here, here, wsend.at[0], wrecv.at[index], grid.device(offset)).wait_recv()
        remote(here, here, wsend.at[1], wrecv.at[len(plane)],
               grid.device((0, 0, 0), 1)).start()
    here = wout.at[:, pl.ds(pl.multiple_of(mine * part, part), part)]
    remote(here, wx.at[mine, grid.core], wsend.at[1], wrecv.at[len(plane)],
           grid.device((0, 0, 0), 1)).start()
    far = grid.device((0, 0, 0), 1)
    other = wx.at[:, 1 - grid.core]
    remote(other, other, wsend.at[1], wrecv.at[len(plane)], far).wait()
    rest = wx.at[pl.ds(0, kv - 1), 0]
    remote(rest, rest, wsend.at[0], wrecv.at[0], far).wait_send()
    for p in range(pieces):
        spread.sent(p, xt.at[p, :, 0], xt.at[p, pl.ds(0, chips - 1), 0])
    wx_out[...] = wx[...]


def project(kv, tp, width, tokens, gain, wq, wk, wv, wz, ws, wd, rate, extra, strength, decay,
            accepted, parent, wo):
    pieces, own, seqs = tokens.shape
    cols = wq.shape[1]
    small = wv.shape[0]
    heads = rate.shape[1]
    chips = kv * tp // 2
    part = wo.shape[1] // kv
    rows = 2 * cols + 2 * small + 16 * -(-2 * heads // 16)
    vmem, anyw = pltpu.VMEM, pl.ANY
    spec = lambda space: pl.BlockSpec(memory_space=space)
    grid = Grid(kv, tp)
    return pl.pallas_call(
        functools.partial(project_kernel, kv, tp),
        in_specs=[spec(s) for s in (
            anyw, vmem, anyw, anyw, anyw, anyw, vmem, vmem, vmem, vmem, vmem, vmem, vmem, vmem, anyw
        )],
        out_specs=[spec(vmem)] * 6,
        out_shape=[
            jax.ShapeDtypeStruct((pieces, seqs, cols), bf16),
            jax.ShapeDtypeStruct((pieces, seqs, cols), bf16),
            jax.ShapeDtypeStruct((pieces, small, seqs), bf16),
            jax.ShapeDtypeStruct((pieces, small, seqs), bf16),
            jax.ShapeDtypeStruct((pieces, heads, 8, seqs), f32),
            jax.ShapeDtypeStruct((kv, 2, wo.shape[0], part), bf16),
        ],
        scratch_shapes=[
            pltpu.VMEM((pieces, chips, 2, own, seqs), bf16),
            pltpu.VMEM((rows, width), bf16),
            pltpu.VMEM((width, 128), f32),
            pltpu.VMEM((2, width, cols), bf16),
            pltpu.VMEM(wo.shape, bf16),
            pltpu.VMEM((kv, 2, wo.shape[0], part), bf16),
            pltpu.SemaphoreType.DMA((6,)),
            pltpu.SemaphoreType.DMA((pieces,)),
            pltpu.SemaphoreType.DMA((pieces, 2, chips)),
            pltpu.SemaphoreType.DMA((2, pieces)),
            pltpu.SemaphoreType.DMA((2,)),
            pltpu.SemaphoreType.DMA((kv,)),
        ],
        compiler_params=pltpu.CompilerParams(
            collective_id=0, has_side_effects=True, vmem_limit_bytes=48 * 1024 * 1024
        ),
        cost_estimate=pl.CostEstimate(
            flops=2 * rows * width * pieces * seqs, bytes_accessed=8 << 20, transcendentals=0
        ),
    )(tokens, gain, wq, wk, wv, wz, ws, wd, rate, extra, strength, decay, accepted, parent, wo)


def total(terms):
    terms = list(terms)
    while len(terms) > 1:
        terms = [sum(terms[i : i + 2][1:], terms[i]) for i in range(0, len(terms), 2)]
    return terms[0]


def delta_kernel(
    prop, q_ref, k_ref, ok_ref, v_ref, ov_ref, z_ref, sc_ref, hg_ref, s_ref,
    o_ref, sq_ref, out_ref, kt_ref, eg_ref,
):
    lanes = s_ref.shape[0]
    vdim = s_ref.shape[2]
    hd = s_ref.shape[3]
    groups = lanes // GROUP

    for index, ref in enumerate((ok_ref, k_ref, q_ref)):
        for p in range(prop):
            tile = ref[p].astype(f32)
            kt_ref[index * prop + p] = tile.T
    positions = 2 * prop
    square = [jnp.sum(kt_ref[i] * kt_ref[i], axis=0, keepdims=True) for i in range(3 * prop)]
    inv = [lax.rsqrt(x + epsilon) for x in square]
    inv = inv[:positions] + [x * hd ** (-0.5) for x in inv[positions:]]

    def scalar(row, p):
        return sc_ref[p, 0, row : row + 1, :]

    beta = [scalar(0, p) for p in range(prop)] + [scalar(2, p) for p in range(prop)]
    g = [scalar(1, p) for p in range(prop)] + [scalar(3, p) for p in range(prop)]
    parents = [scalar(4, p) for p in range(prop)]
    ancestor = []
    for i in range(prop):
        direct = [jnp.where(parents[i] == float(j), 1.0, 0.0) for j in range(i)]
        row = []
        for j in range(i):
            row.append(total([direct[j]] + [direct[m] * ancestor[m][j] for m in range(j + 1, i)]))
        ancestor.append(row)

    def vis(i, j):
        if i < prop or j < prop:
            return None
        return ancestor[i - prop][j - prop]

    gam = []
    for i in range(positions):
        acc = g[i]
        for j in range(i):
            seen = vis(i, j)
            acc = acc + (g[j] if seen is None else seen * g[j])
        gam.append(acc)
    eg = [jnp.exp(x) for x in gam]

    def decay(i, j):
        value = jnp.exp(jnp.minimum(gam[i] - gam[j], 0.0))
        seen = vis(i, j)
        return value if seen is None else value * seen

    def gram(i, j):
        return jnp.sum(kt_ref[i] * kt_ref[j], axis=0, keepdims=True) * (inv[i] * inv[j])

    dec = {(i, j): decay(i, j) for i in range(positions) for j in range(i)}
    coupling = {(i, j): beta[i] * gram(i, j) * dec[i, j] for (i, j) in dec}
    reach = {}
    for p in range(prop):
        i = prop + p
        for j in range(i + 1):
            value = gram(positions + p, j)
            reach[p, j] = value if j == i else value * dec[i, j]

    last = eg[prop - 1]
    eg_ref[...] = jnp.broadcast_to(last, (lanes, lanes)).T

    lane = lax.broadcasted_iota(jnp.int32, (vdim, lanes), 1)
    inner, outer = lane % GROUP, lane // GROUP
    products = []
    for c in range(groups):
        rows = s_ref[c * GROUP : (c + 1) * GROUP, 0].reshape(GROUP * vdim, hd).astype(bf16)
        tiles = []
        for ref in (ok_ref, k_ref, q_ref):
            for p in range(prop):
                start = c * GROUP
                tiles.append(ref[p, start : start + GROUP, :])
        keys = jnp.concatenate(tiles, axis=0)
        product = lax.dot_general(
            rows, keys, (((1,), (1,)), ((), ())), preferred_element_type=f32
        )
        wide = []
        for first in range(0, 3 * prop * GROUP, lanes):
            width = min(lanes, 3 * prop * GROUP - first)
            part = product[:, first : first + width]
            chosen = part[:vdim]
            for s in range(1, GROUP):
                mask = (inner if width == lanes else inner[:, :width]) == s
                chosen = jnp.where(mask, part[s * vdim : (s + 1) * vdim], chosen)
            if width < lanes:
                chosen = jnp.concatenate(
                    [chosen, jnp.zeros((vdim, lanes - width), f32)], axis=1
                )
            wide.append(chosen)
        products.append(wide)

    per_tile = lanes // GROUP

    def swap(source, sources, targets):
        shifted = []
        for d in range(groups):
            acc = None
            for a in range(sources):
                t = (a - d) % groups
                if t >= targets:
                    continue
                acc = source[a] if acc is None else jnp.where(outer == t, source[a], acc)
            shifted.append(acc if acc is None or d == 0 else pltpu.roll(acc, d * GROUP, 1))
        results = []
        for t in range(targets):
            acc = None
            for a in range(sources):
                piece = shifted[(a - t) % groups]
                acc = piece if acc is None else jnp.where(outer == a, piece, acc)
            results.append(acc)
        return results

    raw = []
    for tile in range(len(products[0])):
        count = min(per_tile, 3 * prop - tile * per_tile)
        raw += swap([products[c][tile] for c in range(groups)], groups, count)

    update = []
    for i in range(positions):
        source = ov_ref if i < prop else v_ref
        value = source[i % prop].astype(f32)
        acc = beta[i] * value - (beta[i] * eg[i] * inv[i]) * raw[i]
        for j in range(i):
            acc = acc - coupling[i, j] * update[j]
        update.append(acc)

    for p in range(prop):
        i = prop + p
        acc = (eg[i] * inv[positions + p]) * raw[positions + p]
        for j in range(i + 1):
            acc = acc + reach[p, j] * update[j]
        sq_ref[0, p : p + 1, :] = jnp.sum(acc * acc, axis=0, keepdims=True)
        gate = z_ref[p].astype(f32)
        gate = gate / (1.0 + jnp.exp(-gate))
        o_ref[p] = acc * hg_ref[...] * gate

    weighted = [
        update[j] * (jnp.exp(gam[prop - 1] - gam[j]) * inv[j]) for j in range(prop)
    ]
    compact = swap(weighted, prop, groups)
    width = prop * GROUP
    narrow = inner[:, :width]
    for c in range(groups):
        tiles = [ok_ref[p, c * GROUP : (c + 1) * GROUP, :] for p in range(prop)]
        keys = jnp.concatenate(tiles, axis=0)
        piece = compact[c][:, :width]
        left = jnp.concatenate(
            [jnp.where(narrow == s, piece, 0.0) for s in range(GROUP)], axis=0
        ).astype(bf16)
        delta = jnp.dot(left, keys, preferred_element_type=f32)
        for s in range(GROUP):
            seq = c * GROUP + s
            out_ref[seq, 0] = (
                s_ref[seq, 0] * eg_ref[seq : seq + 1, :hd] + delta[s * vdim : (s + 1) * vdim]
            )


def delta_call(lanes, q, k, ok, v, ov, z, scal, hgain, state):
    seqs, heads, vdim, hd = state.shape
    prop = q.shape[0]
    tiles = seqs // lanes
    natural = pl.BlockSpec((prop, lanes, hd), lambda t, h: (0, t, h))
    turned = pl.BlockSpec((prop, vdim, lanes), lambda t, h: (0, h, t))
    state_spec = pl.BlockSpec((lanes, 1, vdim, hd), lambda t, h: (t, h, 0, 0))
    return pl.pallas_call(
        functools.partial(delta_kernel, prop),
        grid=(tiles, heads),
        in_specs=[
            natural,
            natural,
            natural,
            turned,
            turned,
            turned,
            pl.BlockSpec((prop, 1, 8, lanes), lambda t, h: (0, h, 0, t)),
            pl.BlockSpec((vdim, lanes), lambda t, h: (0, 0)),
            state_spec,
        ],
        out_specs=[
            turned,
            pl.BlockSpec((1, prop, lanes), lambda t, h: (h, 0, t)),
            state_spec,
        ],
        out_shape=[
            jax.ShapeDtypeStruct((prop, heads * vdim, seqs), f32),
            jax.ShapeDtypeStruct((heads, prop, seqs), f32),
            jax.ShapeDtypeStruct(state.shape, f32),
        ],
        scratch_shapes=[
            pltpu.VMEM((3 * prop, hd, lanes), f32),
            pltpu.VMEM((lanes, lanes), f32),
        ],
        compiler_params=pltpu.CompilerParams(vmem_limit_bytes=40 * 1024 * 1024),
        cost_estimate=pl.CostEstimate(
            flops=2 * seqs * heads * vdim * hd * 256,
            bytes_accessed=8 * seqs * heads * vdim * hd,
            transcendentals=0,
        ),
    )(q, k, ok, v, ov, z, scal, hgain, state)


def output_kernel(
    kv, tp, hd,
    m_ref, sq_ref, wx_ref, gain_ref,
    out_ref,
    squares, xb, wt, mine, parts, sums, local, qsend, qrecv, send, recv, both, psend, precv,
    ssend, srecv,
):
    grid = Grid(kv, tp)
    grid.here()
    pieces, chans, seqs = m_ref.shape
    heads = sq_ref.shape[0]
    vdim = chans // heads
    own = out_ref.shape[1]
    feats = wx_ref.shape[3]
    half_width = seqs // 2
    everyone = [(o, f) for o in offsets(grid.sizes) for f in (0, 1)]
    everyone = [e for e in everyone if any(e[0]) or e[1]]
    meet(grid, everyone)

    row = [(o, f) for o, f in everyone if not o[0] and not o[1]]
    column = lax.axis_index("tp")
    for index, (offset, flip) in enumerate(row):
        remote(
            sq_ref, squares.at[column], qsend.at[index], qrecv.at[index],
            grid.device(offset, flip),
        ).start()
    squares[column] = sq_ref[...]
    for first in range(0, kv):
        piece = wx_ref[first].reshape(2 * chans, feats).astype(f32)
        wt[first] = piece.T.astype(bf16)

    def place(p, half, offset, core):
        return xb.at[p, grid.group(offset), core, :, pl.ds(half * half_width, half_width)]

    for index, (offset, flip) in enumerate(row):
        remote(
            sq_ref, squares.at[column], qsend.at[index], qrecv.at[index],
            grid.device(offset, flip),
        ).wait()
    sizes = (grid.z, grid.y, 1)
    spread = Spread(grid, sizes, FLAT, pieces, STAGGER, place, 2, send, recv, both)
    everything = squares[0]
    for index in range(1, tp):
        everything = everything + squares[index]
    scale = lax.rsqrt(everything / hd + epsilon)
    mine_kv = grid.group((0, 0, 0))
    for p in range(pieces):
        turned = [
            m_ref[p, h * vdim : (h + 1) * vdim, :] * scale[h, p : p + 1, :] for h in range(heads)
        ]
        xb[p, mine_kv, grid.core] = jnp.concatenate(turned, axis=0).astype(bf16)
        spread.begin(p)

    line = [(0, 0, c) for c in range(1, grid.x)]
    depth = kv * 2 * chans

    def finish(p):
        spread.shared(p, xb.at[p, :, 1 - grid.core])
        out = None
        for g in range(kv):
            term = jnp.dot(
                wt[g], xb[p, g].reshape(2 * chans, seqs), preferred_element_type=f32
            )
            out = term if out is None else out + term
        parts[p] = out.reshape(feats // own, own, seqs)
        for index, offset in enumerate(line):
            far = grid.shift(offset)[2] * 2 + grid.core
            remote(
                parts.at[p, far], mine.at[p, index], psend.at[p, index], precv.at[p, index],
                grid.device(offset),
            ).start()

    spread.run(finish)
    slot = grid.at[2] * 2 + grid.core
    me = lax.axis_index("kv") * tp + column
    for p in range(pieces):
        acc = parts[p, slot]
        for index, offset in enumerate(line):
            far = grid.shift(offset)[2] * 2 + grid.core
            remote(
                parts.at[p, far], mine.at[p, index], psend.at[p, index], precv.at[p, index],
                grid.device(offset),
            ).wait()
            acc = acc + mine[p, index]
        parts[p, slot] = acc
        sums[me, p : p + 1, :] = jnp.sum(acc * acc, axis=0, keepdims=True)
    for index, (offset, flip) in enumerate(everyone):
        remote(
            sums.at[me], sums.at[me], ssend.at[0], srecv.at[index], grid.device(offset, flip)
        ).start()
    for index, (offset, flip) in enumerate(everyone):
        z, y, x = grid.shift(negated(offset, grid.sizes))
        core = 1 - grid.core if flip else grid.core
        origin = (z * grid.y + y) * tp + x * 2 + core
        remote(
            sums.at[origin], sums.at[origin], ssend.at[0], srecv.at[index],
            grid.device(offset, flip),
        ).wait_recv()
    summed = jnp.sum(sums[...], axis=0)
    final = lax.rsqrt(summed / (kv * tp * own) + epsilon)
    g = gain_ref[...]
    for p in range(pieces):
        out_ref[p] = (parts[p, slot] * final[p : p + 1, :] * g).astype(bf16)
    rest = sums.at[pl.ds(0, kv * tp - 1)]
    far = grid.device((0, 0, 0), 1)
    remote(rest, rest, ssend.at[0], srecv.at[0], far).wait_send()
    for p in range(pieces):
        spread.sent(p, xb.at[p, :, 0], xb.at[p, pl.ds(0, kv - 1), 0])


def output(kv, tp, hd, own, m, sq, wx, gain):
    pieces, chans, seqs = m.shape
    heads = sq.shape[0]
    feats = wx.shape[3]
    x = tp // 2
    spec = pl.BlockSpec(memory_space=pltpu.VMEM)
    peers = kv * tp - 1
    return pl.pallas_call(
        functools.partial(output_kernel, kv, tp, hd),
        in_specs=[spec] * 4,
        out_specs=spec,
        out_shape=jax.ShapeDtypeStruct((pieces, own, seqs), bf16),
        scratch_shapes=[
            pltpu.VMEM((tp, heads, pieces, seqs), f32),
            pltpu.VMEM((pieces, kv, 2, chans, seqs), bf16),
            pltpu.VMEM((kv, feats, 2 * chans), bf16),
            pltpu.VMEM((pieces, max(x - 1, 1), own, seqs), f32),
            pltpu.VMEM((pieces, feats // own, own, seqs), f32),
            pltpu.VMEM((kv * tp, pieces, seqs), f32),
            pltpu.SemaphoreType.DMA((1,)),
            pltpu.SemaphoreType.DMA((tp,)),
            pltpu.SemaphoreType.DMA((tp,)),
            pltpu.SemaphoreType.DMA((pieces,)),
            pltpu.SemaphoreType.DMA((pieces, 2, kv)),
            pltpu.SemaphoreType.DMA((2, pieces)),
            pltpu.SemaphoreType.DMA((pieces, max(x - 1, 1))),
            pltpu.SemaphoreType.DMA((pieces, max(x - 1, 1))),
            pltpu.SemaphoreType.DMA((1,)),
            pltpu.SemaphoreType.DMA((peers,)),
        ],
        compiler_params=pltpu.CompilerParams(
            collective_id=1, has_side_effects=True, vmem_limit_bytes=32 * 1024 * 1024
        ),
        cost_estimate=pl.CostEstimate(
            flops=2 * feats * kv * 2 * chans * pieces * seqs, bytes_accessed=4 << 20,
            transcendentals=0,
        ),
    )(m, sq, wx, gain)


def on_device(
    kv,
    tp,
    tokens,
    input_norm_gain,
    query_weight,
    key_weight,
    value_weight,
    output_gate_weight,
    strength_weight,
    decay_weight,
    head_decay_rate,
    proposal_log_decay,
    head_norm_gain,
    output_weight,
    output_norm_gain,
    state,
    previous_keys,
    previous_values,
    previous_log_decay,
    previous_strengths,
    accepted,
    parent,
):
    seqs, heads, vdim, hd = state.shape
    prop = parent.shape[1]
    width = input_norm_gain.shape[0]
    lanes = min(128, seqs)
    own = tokens.shape[2]
    channels = heads * vdim

    def turn(x):
        return jnp.transpose(x, (1, 2, 0))

    q, k, v, z, scal, wx = project(
        kv, tp, width,
        turn(tokens),
        input_norm_gain[None, :],
        query_weight,
        key_weight,
        turn(value_weight).reshape(channels, width),
        turn(output_gate_weight).reshape(channels, width),
        strength_weight.T,
        decay_weight.T,
        head_decay_rate[None, :],
        turn(proposal_log_decay),
        turn(previous_strengths),
        turn(previous_log_decay),
        accepted[None, :],
        parent.T,
        output_weight.reshape(channels, width),
    )
    old_keys = jnp.transpose(previous_keys, (1, 0, 2))
    old_values = jnp.transpose(previous_values, (1, 2, 3, 0)).reshape(prop, channels, seqs)
    hgain = jnp.broadcast_to(head_norm_gain.astype(f32)[:, None], (vdim, lanes))
    m, sq, accepted_state = delta_call(
        lanes, q, k, old_keys, v, old_values, z, scal, hgain, state
    )
    ogain = jnp.broadcast_to(output_norm_gain.astype(f32)[:, None], (own, seqs))
    layer_out = output(kv, tp, hd, own, m, sq, wx, ogain)
    return (jnp.transpose(layer_out, (2, 0, 1)), accepted_state)


def solution(mesh):
    placed = (
        P(None, None, AXES),
        P(),
        P(None, "kv"),
        P(None, "kv"),
        P(None, "kv", "tp"),
        P(None, "kv", "tp"),
        P(None, "kv"),
        P(None, "kv"),
        P("kv"),
        P(None, None, "kv"),
        P("tp"),
        P("kv", "tp", None),
        P(AXES),
        P(None, "kv", "tp", None),
        P(None, None, "kv"),
        P(None, None, "kv", "tp"),
        P(None, None, "kv"),
        P(None, None, "kv"),
        P(),
        P(),
    )
    return jax.shard_map(
        functools.partial(on_device, mesh.shape["kv"], mesh.shape["tp"]),
        mesh=mesh,
        in_specs=placed,
        out_specs=(P(None, None, AXES), P(None, "kv", "tp", None)),
        check_vma=False,
    )
```

```python
import functools

import jax
import jax.numpy as jnp
from jax import lax
from jax.experimental import pallas as pl
from jax.experimental.pallas import tpu as pltpu
from jax.sharding import PartitionSpec as P

epsilon = 1e-06
GROUP = 16
AXES = ("kv", "tp")
MESH = pl.DeviceIdType.MESH
f32, bf16 = jnp.float32, jnp.bfloat16


class Grid:
    def __init__(self, kv, tp):
        self.kv, self.tp = kv, tp
        self.x = tp // 2
        self.y = self.x if kv % self.x == 0 else 1
        self.z = kv // self.y
        self.sizes = (self.z, self.y, self.x)

    def here(self):
        kv, tp = lax.axis_index("kv"), lax.axis_index("tp")
        self.at = (kv // self.y, lax.rem(kv, self.y), tp // 2)
        self.core = lax.rem(tp, 2)

    def shift(self, offset):
        return tuple(lax.rem(a + o % n, n) for a, o, n in zip(self.at, offset, self.sizes))

    def device(self, offset, flip=0):
        z, y, x = self.shift(offset)
        core = 1 - self.core if flip else self.core
        return (z * self.y + y, x * 2 + core)

    def chip(self, offset):
        z, y, x = self.shift(offset)
        return (z * self.y + y) * self.x + x

    def group(self, offset):
        z, y, _ = self.shift(offset)
        return z * self.y + y


def offsets(sizes):
    return [(a, b, c) for a in range(sizes[0]) for b in range(sizes[1]) for c in range(sizes[2])]


def negated(offset, sizes):
    return tuple(-o % n for o, n in zip(offset, sizes))


def meet(grid, peers):
    peers = set(peers) | {(negated(o, grid.sizes), f) for o, f in peers}
    peers = sorted(peers - {((0, 0, 0), 0)})
    barrier = pltpu.get_barrier_semaphore()
    for offset, flip in peers:
        pl.semaphore_signal(
            barrier, inc=1, device_id=grid.device(offset, flip), device_id_type=MESH
        )
    pl.semaphore_wait(barrier, len(peers))


def remote(src, dst, send, recv, device):
    return pltpu.make_async_remote_copy(
        src_ref=src, dst_ref=dst, send_sem=send, recv_sem=recv, device_id=device,
        device_id_type=MESH,
    )


def tree(sizes, order):
    steps = []
    for offset in offsets(sizes):
        reached = max([order.index(d) + 1 for d in range(3) if offset[d]], default=0)
        onward = [(d, k) for d in order[reached:] for k in range(1, sizes[d])]
        steps.append((offset, onward))
    return steps


def unit(dim, sign):
    return tuple(sign if d == dim else 0 for d in range(3))


def plan(sizes, orders, pieces, stagger):
    events = []
    for p in range(pieces):
        for half, (order, sign) in enumerate(orders):
            for offset, onward in tree(sizes, order):
                level = sum(1 for o in offset if o)
                events.append((level + stagger * p, p, half, offset, onward))
    return sorted(events, key=lambda e: (e[0], e[1], e[3], e[2]))


class Spread:
    def __init__(self, grid, sizes, orders, pieces, stagger, place, halves, send, recv, both):
        self.grid, self.sizes, self.orders, self.pieces = grid, sizes, orders, pieces
        self.place, self.halves = place, halves
        self.send, self.recv, self.both = send, recv, both
        self.events = plan(sizes, orders, pieces, stagger)

    def slot(self, offset):
        a, b, c = offset
        return (a * self.sizes[1] + b) * self.sizes[2] + c

    def source(self, half, offset):
        sign = self.orders[half][1]
        return tuple(-sign * o for o in offset)

    def view(self, p, half, offset):
        return self.place(p, half, self.source(half, offset), self.grid.core)

    def copy(self, p, half, offset, step):
        sign = self.orders[half][1]
        dim, count = step
        landed = tuple(o + (count if d == dim else 0) for d, o in enumerate(offset))
        here = self.view(p, half, offset)
        return remote(
            here, here, self.send.at[p], self.recv.at[p, half, self.slot(landed)],
            self.grid.device(unit(dim, sign * count)),
        )

    def share(self, p, half, offset):
        here = self.view(p, half, offset)
        return remote(
            here, here, self.both.at[0, p], self.both.at[1, p], self.grid.device((0, 0, 0), 1)
        )

    def run(self, finish):
        left = [0] * self.pieces
        for _, p, half, offset, onward in self.events:
            left[p] += 1
        for _, p, half, offset, onward in self.events:
            if any(offset):
                here = self.view(p, half, offset)
                remote(
                    here, here, self.send.at[p], self.recv.at[p, half, self.slot(offset)],
                    self.grid.device((0, 0, 0), 1),
                ).wait_recv()
                for dim in onward:
                    self.copy(p, half, offset, dim).start()
                self.share(p, half, offset).start()
            left[p] -= 1
            if left[p] == 0:
                finish(p)

    def begin(self, p):
        for _, q, half, offset, onward in self.events:
            if q == p and not any(offset):
                for dim in onward:
                    self.copy(p, half, offset, dim).start()
                self.share(p, half, offset).start()

    def shared(self, p, whole):
        remote(whole, whole, self.both.at[0, p], self.both.at[1, p],
               self.grid.device((0, 0, 0), 1)).wait_recv()

    def sent(self, p, whole, rest):
        far = self.grid.device((0, 0, 0), 1)
        remote(rest, rest, self.send.at[p], self.both.at[1, p], far).wait_send()
        remote(whole, whole, self.both.at[0, p], self.both.at[1, p], far).wait_send()


ORDERS = (((0, 1, 2), 1), ((0, 2, 1), -1))
FLAT = (((0, 1, 2), 1), ((0, 1, 2), -1))
STAGGER = 0
VMEM_ALL = 67043328


def project_kernel(
    kv, tp,
    tok, wq, wk, wv, wz, wo, gain_in, ws_in, wd_in, rate_in, extra_in, strength_in, decay_in,
    accepted_in, parent_in, old_in,
    ok_out, q_out, k_out, v_out, z_out, sc_out, wx_out,
    xt, wt, gcol, wqk, wout, wx, gain, ws, wd, rate, extra, old_strength, old_decay, accepted,
    parent, old, local, send, recv, both, wsend, wrecv,
):
    grid = Grid(kv, tp)
    grid.here()
    pieces, own, seqs = tok.shape
    width, cols = wq.shape
    small = wv.shape[0]
    heads = rate.shape[1]
    part = wout.shape[1] // kv
    half_width = seqs // 2

    def place(p, half, offset, core):
        return xt.at[p, grid.chip(offset), core, :, pl.ds(half * half_width, half_width)]

    loads = [
        pltpu.make_async_copy(tok, xt.at[:, grid.chip((0, 0, 0)), grid.core], local.at[0]),
        pltpu.make_async_copy(wo, wout, local.at[1]),
        pltpu.make_async_copy(wq, wqk.at[0], local.at[2]),
        pltpu.make_async_copy(wk, wqk.at[1], local.at[3]),
        pltpu.make_async_copy(wv, wt.at[pl.ds(2 * cols, small)], local.at[4]),
        pltpu.make_async_copy(wz, wt.at[pl.ds(2 * cols + small, small)], local.at[5]),
    ]
    little = zip(
        (gain_in, ws_in, wd_in, rate_in, extra_in, strength_in, decay_in, accepted_in, parent_in,
         old_in),
        (gain, ws, wd, rate, extra, old_strength, old_decay, accepted, parent, old),
    )
    for index, (source, target) in enumerate(little):
        loads.append(pltpu.make_async_copy(source, target, local.at[6 + index]))
    for load in loads:
        load.start()

    plane = [o for o in offsets((grid.z, grid.y, 1)) if any(o)]
    peers = [(unit(d, s), 0) for d in range(3) for s in (1, -1) if grid.sizes[d] > 1]
    peers = [(tuple(o % n for o, n in zip(off, grid.sizes)), f) for off, f in peers]
    peers += [(o, 0) for o in plane] + [((0, 0, 0), 1)]
    meet(grid, peers)

    spread = Spread(
        grid, grid.sizes, ORDERS, pieces, 0.5, place, 2, send, recv, both
    )
    loads[0].wait()
    for p in range(pieces):
        spread.begin(p)
    loads[1].wait()
    mine = grid.group((0, 0, 0))
    for index, offset in enumerate(plane):
        start = pl.multiple_of(grid.group(offset) * part, part)
        remote(
            wout.at[:, pl.ds(start, part)], wx.at[mine, grid.core],
            wsend.at[0], wrecv.at[index], grid.device(offset),
        ).start()
    wx[mine, grid.core] = wout[:, pl.ds(pl.multiple_of(mine * part, part), part)]

    for load in loads[6:]:
        load.wait()
    gains = gain[...].astype(f32)
    for first in range(0, width, 128):
        piece = gains[first // 128 : first // 128 + 1, :]
        gcol[first : first + 128, :] = jnp.broadcast_to(piece, (128, 128)).T
    for p in range(pieces):
        ok_out[p] = old[:, p, :]
    loads[2].wait()
    loads[3].wait()
    for which in range(2):
        for first in range(0, width, 256):
            piece = wqk[which, first : first + 256, :].astype(f32)
            wt[which * cols : (which + 1) * cols, first : first + 256] = piece.T.astype(bf16)
    loads[4].wait()
    loads[5].wait()
    tail = wt.shape[0] - 2 * cols - 2 * small
    rows = [ws[...].astype(f32), wd[...].astype(f32)]
    rows.append(jnp.zeros((tail - 2 * heads, width), f32))
    wt[2 * cols + 2 * small :, :] = jnp.concatenate(rows, axis=0).astype(bf16)

    chips = kv * tp // 2

    def finish(p):
        spread.shared(p, xt.at[p, :, 1 - grid.core])
        x = xt[p].reshape(width, seqs).astype(f32)
        square = jnp.sum(x * x, axis=0, keepdims=True)
        scale = lax.rsqrt(square / width + epsilon)
        g = jnp.concatenate([gcol[...]] * (seqs // 128), axis=1)
        normed = (x * scale * g).astype(bf16)
        out = jnp.dot(wt[...], normed, preferred_element_type=f32)
        for index, ref in enumerate((q_out, k_out)):
            ref[p] = out[index * cols : (index + 1) * cols].T.astype(bf16)
        v_out[p] = out[2 * cols : 2 * cols + small].astype(bf16)
        z_out[p] = out[2 * cols + small : 2 * cols + 2 * small].astype(bf16)
        side = out[2 * cols + 2 * small :]
        live = jnp.where(accepted[...] > p, 1.0, 0.0)
        for h in range(heads):
            strength = side[h : h + 1]
            decay = side[heads + h : heads + h + 1]
            beta = 1.0 / (1.0 + jnp.exp(-strength))
            soft = jnp.maximum(decay, 0.0) + jnp.log1p(jnp.exp(-jnp.abs(decay)))
            g_new = -rate[0:1, h : h + 1] * soft + extra[p, h : h + 1, :]
            zero = jnp.zeros((1, seqs), f32)
            sc_out[p, h] = jnp.concatenate(
                [
                    old_strength[p, h : h + 1, :] * live,
                    old_decay[p, h : h + 1, :] * live,
                    beta,
                    g_new,
                    parent[p : p + 1, :].astype(f32),
                    zero, zero, zero,
                ],
                axis=0,
            )

    spread.run(finish)

    for index, offset in enumerate(plane):
        origin = grid.group(negated(offset, grid.sizes))
        here = wx.at[origin, grid.core]
        remote(here, here, wsend.at[0], wrecv.at[index], grid.device(offset)).wait_recv()
        remote(here, here, wsend.at[1], wrecv.at[len(plane)],
               grid.device((0, 0, 0), 1)).start()
    here = wout.at[:, pl.ds(pl.multiple_of(mine * part, part), part)]
    remote(here, wx.at[mine, grid.core], wsend.at[1], wrecv.at[len(plane)],
           grid.device((0, 0, 0), 1)).start()
    far = grid.device((0, 0, 0), 1)
    other = wx.at[:, 1 - grid.core]
    remote(other, other, wsend.at[1], wrecv.at[len(plane)], far).wait()
    rest = wx.at[pl.ds(0, kv - 1), 0]
    remote(rest, rest, wsend.at[0], wrecv.at[0], far).wait_send()
    for p in range(pieces):
        spread.sent(p, xt.at[p, :, 0], xt.at[p, pl.ds(0, chips - 1), 0])
    wx_out[...] = wx[...]


def project(kv, tp, *args):
    tokens, wq, _, wv, _, wo, gain, _, _, rate = args[:10]
    pieces, own, seqs = tokens.shape
    width, cols = wq.shape
    small = wv.shape[0]
    heads = rate.shape[1]
    chips = kv * tp // 2
    part = wo.shape[1] // kv
    rows = 2 * cols + 2 * small + 16 * -(-2 * heads // 16)
    return pl.pallas_call(
        functools.partial(project_kernel, kv, tp),
        in_specs=[pl.BlockSpec(memory_space=pltpu.HBM)] * len(args),
        out_specs=[pl.BlockSpec(memory_space=pltpu.VMEM)] * 7,
        out_shape=[
            jax.ShapeDtypeStruct((pieces, seqs, cols), bf16),
            jax.ShapeDtypeStruct((pieces, seqs, cols), bf16),
            jax.ShapeDtypeStruct((pieces, seqs, cols), bf16),
            jax.ShapeDtypeStruct((pieces, small, seqs), bf16),
            jax.ShapeDtypeStruct((pieces, small, seqs), bf16),
            jax.ShapeDtypeStruct((pieces, heads, 8, seqs), f32),
            jax.ShapeDtypeStruct((kv, 2, wo.shape[0], part), bf16),
        ],
        scratch_shapes=[
            pltpu.VMEM((pieces, chips, 2, own, seqs), bf16),
            pltpu.VMEM((rows, width), bf16),
            pltpu.VMEM((width, 128), f32),
            pltpu.VMEM((2, width, cols), bf16),
            pltpu.VMEM(wo.shape, bf16),
            pltpu.VMEM((kv, 2, wo.shape[0], part), bf16),
        ]
        + [pltpu.VMEM(x.shape, x.dtype) for x in args[6:]]
        + [
            pltpu.SemaphoreType.DMA((len(args),)),
            pltpu.SemaphoreType.DMA((pieces,)),
            pltpu.SemaphoreType.DMA((pieces, 2, chips)),
            pltpu.SemaphoreType.DMA((2, pieces)),
            pltpu.SemaphoreType.DMA((2,)),
            pltpu.SemaphoreType.DMA((kv,)),
        ],
        compiler_params=pltpu.CompilerParams(
            collective_id=0, has_side_effects=True, vmem_limit_bytes=VMEM_ALL
        ),
        cost_estimate=pl.CostEstimate(
            flops=2 * rows * width * pieces * seqs, bytes_accessed=8 << 20, transcendentals=0
        ),
    )(*args)


def column(row):
    size = row.shape[1]
    square = (size, size)
    chosen = lax.broadcasted_iota(jnp.int32, square, 0) == lax.broadcasted_iota(jnp.int32, square, 1)
    wide = jnp.broadcast_to(row.astype(f32), square)
    return jnp.sum(jnp.where(chosen, wide, 0.0), axis=1, keepdims=True)


def total(terms):
    terms = list(terms)
    while len(terms) > 1:
        terms = [sum(terms[i : i + 2][1:], terms[i]) for i in range(0, len(terms), 2)]
    return terms[0]


def delta_kernel(
    prop, q_ref, k_ref, ok_ref, v_ref, ov_ref, z_ref, sc_ref, hg_ref, s_ref,
    o_ref, sq_ref, out_ref, kt_ref, eg_ref,
):
    lanes = s_ref.shape[0]
    vdim = s_ref.shape[2]
    hd = s_ref.shape[3]
    groups = lanes // GROUP

    for index, ref in enumerate((ok_ref, k_ref, q_ref)):
        for p in range(prop):
            tile = ref[p].astype(f32)
            kt_ref[index * prop + p] = tile.T
    positions = 2 * prop
    square = [jnp.sum(kt_ref[i] * kt_ref[i], axis=0, keepdims=True) for i in range(3 * prop)]
    inv = [lax.rsqrt(x + epsilon) for x in square]
    inv = inv[:positions] + [x * hd ** (-0.5) for x in inv[positions:]]

    def scalar(row, p):
        return sc_ref[p, 0, row : row + 1, :]

    beta = [scalar(0, p) for p in range(prop)] + [scalar(2, p) for p in range(prop)]
    g = [scalar(1, p) for p in range(prop)] + [scalar(3, p) for p in range(prop)]
    parents = [scalar(4, p) for p in range(prop)]
    ancestor = []
    for i in range(prop):
        direct = [jnp.where(parents[i] == float(j), 1.0, 0.0) for j in range(i)]
        row = []
        for j in range(i):
            row.append(total([direct[j]] + [direct[m] * ancestor[m][j] for m in range(j + 1, i)]))
        ancestor.append(row)

    def vis(i, j):
        if i < prop or j < prop:
            return None
        return ancestor[i - prop][j - prop]

    gam = []
    for i in range(positions):
        acc = g[i]
        for j in range(i):
            seen = vis(i, j)
            acc = acc + (g[j] if seen is None else seen * g[j])
        gam.append(acc)
    eg = [jnp.exp(x) for x in gam]

    def decay(i, j):
        value = jnp.exp(jnp.minimum(gam[i] - gam[j], 0.0))
        seen = vis(i, j)
        return value if seen is None else value * seen

    def gram(i, j):
        return jnp.sum(kt_ref[i] * kt_ref[j], axis=0, keepdims=True) * (inv[i] * inv[j])

    dec = {(i, j): decay(i, j) for i in range(positions) for j in range(i)}
    coupling = {(i, j): beta[i] * gram(i, j) * dec[i, j] for (i, j) in dec}
    reach = {}
    for p in range(prop):
        i = prop + p
        for j in range(i + 1):
            value = gram(positions + p, j)
            reach[p, j] = value if j == i else value * dec[i, j]

    last = eg[prop - 1]
    eg_ref[...] = jnp.broadcast_to(last, (lanes, lanes)).T

    lane = lax.broadcasted_iota(jnp.int32, (vdim, lanes), 1)
    inner, outer = lane % GROUP, lane // GROUP
    products = []
    for c in range(groups):
        rows = s_ref[c * GROUP : (c + 1) * GROUP, 0].reshape(GROUP * vdim, hd).astype(bf16)
        tiles = []
        for ref in (ok_ref, k_ref, q_ref):
            for p in range(prop):
                start = c * GROUP
                tiles.append(ref[p, start : start + GROUP, :])
        keys = jnp.concatenate(tiles, axis=0)
        product = lax.dot_general(
            rows, keys, (((1,), (1,)), ((), ())), preferred_element_type=f32
        )
        wide = []
        for first in range(0, 3 * prop * GROUP, lanes):
            width = min(lanes, 3 * prop * GROUP - first)
            part = product[:, first : first + width]
            chosen = part[:vdim]
            for s in range(1, GROUP):
                mask = (inner if width == lanes else inner[:, :width]) == s
                chosen = jnp.where(mask, part[s * vdim : (s + 1) * vdim], chosen)
            if width < lanes:
                chosen = jnp.concatenate(
                    [chosen, jnp.zeros((vdim, lanes - width), f32)], axis=1
                )
            wide.append(chosen)
        products.append(wide)

    per_tile = lanes // GROUP

    def swap(source, sources, targets):
        shifted = []
        for d in range(groups):
            acc = None
            for a in range(sources):
                t = (a - d) % groups
                if t >= targets:
                    continue
                acc = source[a] if acc is None else jnp.where(outer == t, source[a], acc)
            shifted.append(acc if acc is None or d == 0 else pltpu.roll(acc, d * GROUP, 1))
        results = []
        for t in range(targets):
            acc = None
            for a in range(sources):
                piece = shifted[(a - t) % groups]
                acc = piece if acc is None else jnp.where(outer == a, piece, acc)
            results.append(acc)
        return results

    raw = []
    for tile in range(len(products[0])):
        count = min(per_tile, 3 * prop - tile * per_tile)
        raw += swap([products[c][tile] for c in range(groups)], groups, count)

    update = []
    for i in range(positions):
        source = ov_ref if i < prop else v_ref
        value = source[i % prop].astype(f32)
        acc = beta[i] * value - (beta[i] * eg[i] * inv[i]) * raw[i]
        for j in range(i):
            acc = acc - coupling[i, j] * update[j]
        update.append(acc)

    hgain = column(hg_ref[...])
    for p in range(prop):
        i = prop + p
        acc = (eg[i] * inv[positions + p]) * raw[positions + p]
        for j in range(i + 1):
            acc = acc + reach[p, j] * update[j]
        sq_ref[0, p : p + 1, :] = jnp.sum(acc * acc, axis=0, keepdims=True)
        gate = z_ref[p].astype(f32)
        gate = gate / (1.0 + jnp.exp(-gate))
        o_ref[p] = acc * hgain * gate

    weighted = [
        update[j] * (jnp.exp(gam[prop - 1] - gam[j]) * inv[j]) for j in range(prop)
    ]
    compact = swap(weighted, prop, groups)
    width = prop * GROUP
    narrow = inner[:, :width]
    for c in range(groups):
        tiles = [ok_ref[p, c * GROUP : (c + 1) * GROUP, :] for p in range(prop)]
        keys = jnp.concatenate(tiles, axis=0)
        piece = compact[c][:, :width]
        left = jnp.concatenate(
            [jnp.where(narrow == s, piece, 0.0) for s in range(GROUP)], axis=0
        ).astype(bf16)
        delta = jnp.dot(left, keys, preferred_element_type=f32)
        for s in range(GROUP):
            seq = c * GROUP + s
            out_ref[seq, 0] = (
                s_ref[seq, 0] * eg_ref[seq : seq + 1, :hd] + delta[s * vdim : (s + 1) * vdim]
            )


def delta_call(lanes, q, k, ok, v, ov, z, scal, hgain, state):
    seqs, heads, vdim, hd = state.shape
    prop = q.shape[0]
    tiles = seqs // lanes
    natural = pl.BlockSpec((prop, lanes, hd), lambda t, h: (0, t, h))
    turned = pl.BlockSpec((prop, vdim, lanes), lambda t, h: (0, h, t))
    state_spec = pl.BlockSpec((lanes, 1, vdim, hd), lambda t, h: (t, h, 0, 0))
    return pl.pallas_call(
        functools.partial(delta_kernel, prop),
        grid=(tiles, heads),
        in_specs=[
            natural,
            natural,
            natural,
            turned,
            turned,
            turned,
            pl.BlockSpec((prop, 1, 8, lanes), lambda t, h: (0, h, 0, t)),
            pl.BlockSpec((1, vdim), lambda t, h: (0, 0)),
            state_spec,
        ],
        out_specs=[
            turned,
            pl.BlockSpec((1, prop, lanes), lambda t, h: (h, 0, t)),
            state_spec,
        ],
        out_shape=[
            jax.ShapeDtypeStruct((prop, heads * vdim, seqs), f32),
            jax.ShapeDtypeStruct((heads, prop, seqs), f32),
            jax.ShapeDtypeStruct(state.shape, f32),
        ],
        scratch_shapes=[
            pltpu.VMEM((3 * prop, hd, lanes), f32),
            pltpu.VMEM((lanes, lanes), f32),
        ],
        compiler_params=pltpu.CompilerParams(vmem_limit_bytes=VMEM_ALL - (400 << 10)),
        cost_estimate=pl.CostEstimate(
            flops=2 * seqs * heads * vdim * hd * 256,
            bytes_accessed=8 * seqs * heads * vdim * hd,
            transcendentals=0,
        ),
    )(q, k, ok, v, ov, z, scal, hgain, state)


def output_kernel(
    kv, tp, hd,
    m_ref, sq_ref, wx_ref, gain_ref,
    out_ref,
    squares, xb, wt, mine, parts, sums, local, qsend, qrecv, send, recv, both, psend, precv,
    ssend, srecv,
):
    grid = Grid(kv, tp)
    grid.here()
    pieces, chans, seqs = m_ref.shape
    heads = sq_ref.shape[0]
    vdim = chans // heads
    own = out_ref.shape[1]
    feats = wx_ref.shape[3]
    half_width = seqs // 2
    everyone = [(o, f) for o in offsets(grid.sizes) for f in (0, 1)]
    everyone = [e for e in everyone if any(e[0]) or e[1]]
    meet(grid, everyone)

    row = [(o, f) for o, f in everyone if not o[0] and not o[1]]
    lane = lax.axis_index("tp")
    for index, (offset, flip) in enumerate(row):
        remote(
            sq_ref, squares.at[lane], qsend.at[index], qrecv.at[index],
            grid.device(offset, flip),
        ).start()
    squares[lane] = sq_ref[...]
    for first in range(0, kv):
        piece = wx_ref[first].reshape(2 * chans, feats).astype(f32)
        wt[first] = piece.T.astype(bf16)

    def place(p, half, offset, core):
        return xb.at[p, grid.group(offset), core, :, pl.ds(half * half_width, half_width)]

    for index, (offset, flip) in enumerate(row):
        remote(
            sq_ref, squares.at[lane], qsend.at[index], qrecv.at[index],
            grid.device(offset, flip),
        ).wait()
    sizes = (grid.z, grid.y, 1)
    spread = Spread(grid, sizes, FLAT, pieces, STAGGER, place, 2, send, recv, both)
    everything = squares[0]
    for index in range(1, tp):
        everything = everything + squares[index]
    scale = lax.rsqrt(everything / hd + epsilon)
    mine_kv = grid.group((0, 0, 0))
    for p in range(pieces):
        turned = [
            m_ref[p, h * vdim : (h + 1) * vdim, :] * scale[h, p : p + 1, :] for h in range(heads)
        ]
        xb[p, mine_kv, grid.core] = jnp.concatenate(turned, axis=0).astype(bf16)
        spread.begin(p)

    line = [(0, 0, c) for c in range(1, grid.x)]
    depth = kv * 2 * chans

    def finish(p):
        spread.shared(p, xb.at[p, :, 1 - grid.core])
        out = None
        for g in range(kv):
            term = jnp.dot(
                wt[g], xb[p, g].reshape(2 * chans, seqs), preferred_element_type=f32
            )
            out = term if out is None else out + term
        parts[p] = out.reshape(feats // own, own, seqs)
        for index, offset in enumerate(line):
            far = grid.shift(offset)[2] * 2 + grid.core
            remote(
                parts.at[p, far], mine.at[p, index], psend.at[p, index], precv.at[p, index],
                grid.device(offset),
            ).start()

    spread.run(finish)
    slot = grid.at[2] * 2 + grid.core
    me = lax.axis_index("kv") * tp + lane
    for p in range(pieces):
        acc = parts[p, slot]
        for index, offset in enumerate(line):
            far = grid.shift(offset)[2] * 2 + grid.core
            remote(
                parts.at[p, far], mine.at[p, index], psend.at[p, index], precv.at[p, index],
                grid.device(offset),
            ).wait()
            acc = acc + mine[p, index]
        parts[p, slot] = acc
        sums[me, p : p + 1, :] = jnp.sum(acc * acc, axis=0, keepdims=True)
    for index, (offset, flip) in enumerate(everyone):
        remote(
            sums.at[me], sums.at[me], ssend.at[0], srecv.at[index], grid.device(offset, flip)
        ).start()
    for index, (offset, flip) in enumerate(everyone):
        z, y, x = grid.shift(negated(offset, grid.sizes))
        core = 1 - grid.core if flip else grid.core
        origin = (z * grid.y + y) * tp + x * 2 + core
        remote(
            sums.at[origin], sums.at[origin], ssend.at[0], srecv.at[index],
            grid.device(offset, flip),
        ).wait_recv()
    summed = jnp.sum(sums[...], axis=0)
    final = lax.rsqrt(summed / (kv * tp * own) + epsilon)
    g = column(gain_ref[...])
    for p in range(pieces):
        out_ref[p] = (parts[p, slot] * final[p : p + 1, :] * g).astype(bf16)
    rest = sums.at[pl.ds(0, kv * tp - 1)]
    far = grid.device((0, 0, 0), 1)
    remote(rest, rest, ssend.at[0], srecv.at[0], far).wait_send()
    for p in range(pieces):
        spread.sent(p, xb.at[p, :, 0], xb.at[p, pl.ds(0, kv - 1), 0])


def output(kv, tp, hd, own, m, sq, wx, gain):
    pieces, chans, seqs = m.shape
    heads = sq.shape[0]
    feats = wx.shape[3]
    x = tp // 2
    spec = pl.BlockSpec(memory_space=pltpu.VMEM)
    peers = kv * tp - 1
    return pl.pallas_call(
        functools.partial(output_kernel, kv, tp, hd),
        in_specs=[spec] * 4,
        out_specs=spec,
        out_shape=jax.ShapeDtypeStruct((pieces, own, seqs), bf16),
        scratch_shapes=[
            pltpu.VMEM((tp, heads, pieces, seqs), f32),
            pltpu.VMEM((pieces, kv, 2, chans, seqs), bf16),
            pltpu.VMEM((kv, feats, 2 * chans), bf16),
            pltpu.VMEM((pieces, max(x - 1, 1), own, seqs), f32),
            pltpu.VMEM((pieces, feats // own, own, seqs), f32),
            pltpu.VMEM((kv * tp, pieces, seqs), f32),
            pltpu.SemaphoreType.DMA((1,)),
            pltpu.SemaphoreType.DMA((tp,)),
            pltpu.SemaphoreType.DMA((tp,)),
            pltpu.SemaphoreType.DMA((pieces,)),
            pltpu.SemaphoreType.DMA((pieces, 2, kv)),
            pltpu.SemaphoreType.DMA((2, pieces)),
            pltpu.SemaphoreType.DMA((pieces, max(x - 1, 1))),
            pltpu.SemaphoreType.DMA((pieces, max(x - 1, 1))),
            pltpu.SemaphoreType.DMA((1,)),
            pltpu.SemaphoreType.DMA((peers,)),
        ],
        compiler_params=pltpu.CompilerParams(
            collective_id=1, has_side_effects=True, vmem_limit_bytes=VMEM_ALL - (200 << 10)
        ),
        cost_estimate=pl.CostEstimate(
            flops=2 * feats * kv * 2 * chans * pieces * seqs, bytes_accessed=4 << 20,
            transcendentals=0,
        ),
    )(m, sq, wx, gain)


def on_device(
    kv,
    tp,
    tokens,
    input_norm_gain,
    query_weight,
    key_weight,
    value_weight,
    output_gate_weight,
    strength_weight,
    decay_weight,
    head_decay_rate,
    proposal_log_decay,
    head_norm_gain,
    output_weight,
    output_norm_gain,
    state,
    previous_keys,
    previous_values,
    previous_log_decay,
    previous_strengths,
    accepted,
    parent,
):
    seqs, heads, vdim, hd = state.shape
    prop = parent.shape[1]
    width = input_norm_gain.shape[0]
    lanes = min(128, seqs)
    own = tokens.shape[2]
    channels = heads * vdim

    def turn(x):
        return jnp.transpose(x, (1, 2, 0))

    old_keys, q, k, v, z, scal, wx = project(
        kv, tp,
        turn(tokens),
        query_weight,
        key_weight,
        turn(value_weight).reshape(channels, width),
        turn(output_gate_weight).reshape(channels, width),
        output_weight.reshape(channels, width),
        input_norm_gain.reshape(width // 128, 128),
        strength_weight.T,
        decay_weight.T,
        head_decay_rate[None, :],
        turn(proposal_log_decay),
        turn(previous_strengths),
        turn(previous_log_decay),
        accepted[None, :],
        parent.T,
        previous_keys,
    )
    old_values = jnp.transpose(previous_values, (1, 2, 3, 0)).reshape(prop, channels, seqs)
    m, sq, accepted_state = delta_call(
        lanes, q, k, old_keys, v, old_values, z, scal, head_norm_gain[None, :], state
    )
    layer_out = output(kv, tp, hd, own, m, sq, wx, output_norm_gain[None, :])
    return (jnp.transpose(layer_out, (2, 0, 1)), accepted_state)


def solution(mesh):
    placed = (
        P(None, None, AXES),
        P(),
        P(None, "kv"),
        P(None, "kv"),
        P(None, "kv", "tp"),
        P(None, "kv", "tp"),
        P(None, "kv"),
        P(None, "kv"),
        P("kv"),
        P(None, None, "kv"),
        P("tp"),
        P("kv", "tp", None),
        P(AXES),
        P(None, "kv", "tp", None),
        P(None, None, "kv"),
        P(None, None, "kv", "tp"),
        P(None, None, "kv"),
        P(None, None, "kv"),
        P(),
        P(),
    )
    return jax.shard_map(
        functools.partial(on_device, mesh.shape["kv"], mesh.shape["tp"]),
        mesh=mesh,
        in_specs=placed,
        out_specs=(P(None, None, AXES), P(None, "kv", "tp", None)),
        check_vma=False,
    )
```

```python
import functools

import jax
import jax.numpy as jnp
from jax import lax
from jax.experimental import pallas as pl
from jax.experimental.pallas import tpu as pltpu
from jax.sharding import PartitionSpec as P

epsilon = 1e-06
GROUP = 16
AXES = ("kv", "tp")
MESH = pl.DeviceIdType.MESH
f32, bf16 = jnp.float32, jnp.bfloat16


class Grid:
    def __init__(self, kv, tp):
        self.kv, self.tp = kv, tp
        self.x = tp // 2
        self.y = self.x if kv % self.x == 0 else 1
        self.z = kv // self.y
        self.sizes = (self.z, self.y, self.x)

    def here(self):
        kv, tp = lax.axis_index("kv"), lax.axis_index("tp")
        self.at = (kv // self.y, lax.rem(kv, self.y), tp // 2)
        self.core = lax.rem(tp, 2)

    def shift(self, offset):
        return tuple(lax.rem(a + o % n, n) for a, o, n in zip(self.at, offset, self.sizes))

    def device(self, offset, flip=0):
        z, y, x = self.shift(offset)
        core = 1 - self.core if flip else self.core
        return (z * self.y + y, x * 2 + core)

    def chip(self, offset):
        z, y, x = self.shift(offset)
        return (z * self.y + y) * self.x + x

    def group(self, offset):
        z, y, _ = self.shift(offset)
        return z * self.y + y


def offsets(sizes):
    return [(a, b, c) for a in range(sizes[0]) for b in range(sizes[1]) for c in range(sizes[2])]


def negated(offset, sizes):
    return tuple(-o % n for o, n in zip(offset, sizes))


def meet(grid, peers):
    barrier = pltpu.get_barrier_semaphore()
    for offset, flip in peers:
        pl.semaphore_signal(
            barrier, inc=1, device_id=grid.device(offset, flip), device_id_type=MESH
        )
    pl.semaphore_wait(barrier, len(peers))


def remote(src, dst, send, recv, device):
    return pltpu.make_async_remote_copy(
        src_ref=src, dst_ref=dst, send_sem=send, recv_sem=recv, device_id=device,
        device_id_type=MESH,
    )


def tree(sizes, order):
    steps = []
    for offset in offsets(sizes):
        reached = max([order.index(d) + 1 for d in range(3) if offset[d]], default=0)
        onward = [(d, k) for d in order[reached:] for k in range(1, sizes[d])]
        steps.append((offset, onward))
    return steps


def unit(dim, sign):
    return tuple(sign if d == dim else 0 for d in range(3))


class Spread:
    def __init__(self, grid, sizes, orders, place, send, recv, both):
        self.grid, self.sizes, self.orders = grid, sizes, orders
        self.place, self.send, self.recv, self.both = place, send, recv, both

    def slot(self, offset):
        a, b, c = offset
        return (a * self.sizes[1] + b) * self.sizes[2] + c

    def view(self, u, half, offset):
        sign = self.orders[half][1]
        return self.place(u, half, tuple(-sign * o for o in offset), self.grid.core)

    def pass_on(self, u, half, offset, onward):
        sign = self.orders[half][1]
        here = self.view(u, half, offset)
        for dim, count in onward:
            landed = tuple(o + (count if d == dim else 0) for d, o in enumerate(offset))
            remote(
                here, here, self.send.at[u], self.recv.at[u, half, self.slot(landed)],
                self.grid.device(unit(dim, sign * count)),
            ).start()
        remote(
            here, here, self.both.at[0, u], self.both.at[1, u], self.grid.device((0, 0, 0), 1)
        ).start()

    def begin(self, u):
        for half, (order, _) in enumerate(self.orders):
            for offset, onward in tree(self.sizes, order):
                if not any(offset):
                    self.pass_on(u, half, offset, onward)

    def level(self, u, wanted):
        for half, (order, _) in enumerate(self.orders):
            for offset, onward in tree(self.sizes, order):
                if sum(1 for o in offset if o) != wanted:
                    continue
                here = self.view(u, half, offset)
                remote(
                    here, here, self.send.at[u], self.recv.at[u, half, self.slot(offset)],
                    self.grid.device((0, 0, 0), 1),
                ).wait_recv()
                self.pass_on(u, half, offset, onward)

    def shared(self, u, whole):
        remote(whole, whole, self.both.at[0, u], self.both.at[1, u],
               self.grid.device((0, 0, 0), 1)).wait_recv()

    def sent(self, u, whole, rest):
        far = self.grid.device((0, 0, 0), 1)
        remote(rest, rest, self.send.at[u], self.both.at[1, u], far).wait_send()
        remote(whole, whole, self.both.at[0, u], self.both.at[1, u], far).wait_send()


ORDERS = (((0, 1, 2), 1), ((0, 2, 1), -1))
FLAT = (((0, 1, 2), 1),)
VMEM_ALL = 67043328
LANES = 128


def column(row):
    size = row.shape[1]
    square = (size, size)
    chosen = lax.broadcasted_iota(jnp.int32, square, 0) == lax.broadcasted_iota(jnp.int32, square, 1)
    wide = jnp.broadcast_to(row.astype(f32), square)
    return jnp.sum(jnp.where(chosen, wide, 0.0), axis=1, keepdims=True)


def total(terms):
    terms = list(terms)
    while len(terms) > 1:
        terms = [sum(terms[i : i + 2][1:], terms[i]) for i in range(0, len(terms), 2)]
    return terms[0]


def swap(outer, groups, source, sources, targets):
    shifted = []
    for d in range(groups):
        acc = None
        for a in range(sources):
            t = (a - d) % groups
            if t >= targets:
                continue
            acc = source[a] if acc is None else jnp.where(outer == t, source[a], acc)
        shifted.append(acc if acc is None or d == 0 else pltpu.roll(acc, d * GROUP, 1))
    results = []
    for t in range(targets):
        acc = None
        for a in range(sources):
            piece = shifted[(a - t) % groups]
            acc = piece if acc is None else jnp.where(outer == a, piece, acc)
        results.append(acc)
    return results


def read_state(st, start, h, tiles_of, count):
    vdim, hd = st.shape[2], st.shape[3]
    groups = LANES // GROUP
    lane = lax.broadcasted_iota(jnp.int32, (vdim, LANES), 1)
    inner, outer = lane % GROUP, lane // GROUP
    products = []
    for c in range(groups):
        first = start + c * GROUP
        rows = st[first : first + GROUP, h].reshape(GROUP * vdim, hd).astype(bf16)
        keys = jnp.concatenate(tiles_of(first), axis=0)
        product = lax.dot_general(
            rows, keys, (((1,), (1,)), ((), ())), preferred_element_type=f32
        )
        width = count * GROUP
        chosen = product[:vdim]
        for s in range(1, GROUP):
            chosen = jnp.where(
                inner[:, :width] == s, product[s * vdim : (s + 1) * vdim], chosen
            )
        if width < LANES:
            chosen = jnp.concatenate([chosen, jnp.zeros((vdim, LANES - width), f32)], axis=1)
        products.append(chosen)
    return swap(outer, groups, products, groups, count)


def advance(st, ok, kt, ov, strength, decay, accepted, t, h):
    prop, _, _ = ok.shape
    vdim, hd = st.shape[2], st.shape[3]
    start = t * LANES
    span = slice(start, start + LANES)
    cols = slice(h * hd, (h + 1) * hd)
    groups = LANES // GROUP
    for p in range(prop):
        kt[p] = ok[p, span, cols].astype(f32).T
    inv = [lax.rsqrt(jnp.sum(kt[p] * kt[p], axis=0, keepdims=True) + epsilon) for p in range(prop)]
    count = accepted[:, span]
    live = [jnp.where(count > p, 1.0, 0.0) for p in range(prop)]
    beta = [strength[p, h : h + 1, span] * live[p] for p in range(prop)]
    gam = []
    for p in range(prop):
        step = decay[p, h : h + 1, span] * live[p]
        gam.append(step if p == 0 else gam[-1] + step)
    raw = read_state(
        st, start, h, lambda first: [ok[p, first : first + GROUP, cols] for p in range(prop)], prop
    )
    update = []
    for i in range(prop):
        value = ov[i, h * vdim : (h + 1) * vdim, span].astype(f32)
        acc = beta[i] * value - (beta[i] * jnp.exp(gam[i]) * inv[i]) * raw[i]
        for j in range(i):
            gram = jnp.sum(kt[i] * kt[j], axis=0, keepdims=True) * (inv[i] * inv[j])
            acc = acc - (beta[i] * gram * jnp.exp(jnp.minimum(gam[i] - gam[j], 0.0))) * update[j]
        update.append(acc)
    weighted = [update[j] * (jnp.exp(gam[-1] - gam[j]) * inv[j]) for j in range(prop)]
    lane = lax.broadcasted_iota(jnp.int32, (vdim, LANES), 1)
    inner, outer = lane % GROUP, lane // GROUP
    compact = swap(outer, groups, weighted, prop, groups)
    width = prop * GROUP
    narrow = inner[:, :width]
    fade = jnp.broadcast_to(jnp.exp(gam[-1]), (LANES, LANES)).T
    for c in range(groups):
        first = start + c * GROUP
        keys = jnp.concatenate([ok[p, first : first + GROUP, cols] for p in range(prop)], axis=0)
        piece = compact[c][:, :width]
        left = jnp.concatenate(
            [jnp.where(narrow == s, piece, 0.0) for s in range(GROUP)], axis=0
        ).astype(bf16)
        delta = jnp.dot(left, keys, preferred_element_type=f32)
        for s in range(GROUP):
            seq = c * GROUP + s
            st[start + seq, h] = (
                st[start + seq, h] * fade[seq : seq + 1, :hd] + delta[s * vdim : (s + 1) * vdim]
            )


def propose(st, natural, turned, sc, vz, hgain, m, sq, t, h):
    prop = natural.shape[1]
    vdim, hd = st.shape[2], st.shape[3]
    start = t * LANES
    span = slice(start, start + LANES)
    cols = slice(h * hd, (h + 1) * hd)
    vrows = slice(h * vdim, (h + 1) * vdim)

    def vector(which, p):
        return turned[which, p, cols, span]

    def dot(a, b):
        return jnp.sum(vector(*a) * vector(*b), axis=0, keepdims=True)

    inv_q = [
        lax.rsqrt(dot((0, p), (0, p)) + epsilon) * hd ** (-0.5) for p in range(prop)
    ]
    inv = [lax.rsqrt(dot((1, p), (1, p)) + epsilon) for p in range(prop)]
    beta = [sc[p, h, 0:1, span] for p in range(prop)]
    g = [sc[p, h, 1:2, span] for p in range(prop)]
    parents = [sc[p, h, 2:3, span] for p in range(prop)]
    ancestor = []
    for i in range(prop):
        direct = [jnp.where(parents[i] == float(j), 1.0, 0.0) for j in range(i)]
        row = []
        for j in range(i):
            row.append(total([direct[j]] + [direct[k] * ancestor[k][j] for k in range(j + 1, i)]))
        ancestor.append(row)
    gam = []
    for i in range(prop):
        gam.append(total([g[i]] + [ancestor[i][j] * g[j] for j in range(i)]))
    dec = {
        (i, j): jnp.exp(jnp.minimum(gam[i] - gam[j], 0.0)) * ancestor[i][j]
        for i in range(prop)
        for j in range(i)
    }
    raw = read_state(
        st, start, h,
        lambda first: [
            natural[which, p, first : first + GROUP, cols] for which in (1, 0) for p in range(prop)
        ],
        2 * prop,
    )
    update = []
    for i in range(prop):
        value = vz[0, i, vrows, span].astype(f32)
        acc = beta[i] * value - (beta[i] * jnp.exp(gam[i]) * inv[i]) * raw[i]
        for j in range(i):
            gram = dot((1, i), (1, j)) * (inv[i] * inv[j])
            acc = acc - (beta[i] * gram * dec[i, j]) * update[j]
        update.append(acc)
    for p in range(prop):
        acc = (jnp.exp(gam[p]) * inv_q[p]) * raw[prop + p]
        for j in range(p + 1):
            weight = dot((0, p), (1, j)) * (inv_q[p] * inv[j])
            acc = acc + (weight if j == p else weight * dec[p, j]) * update[j]
        sq[t, h * prop + p : h * prop + p + 1, :] = jnp.sum(acc * acc, axis=0, keepdims=True)
        gate = vz[1, p, vrows, span].astype(f32)
        m[p, vrows, span] = acc * hgain * (gate / (1.0 + jnp.exp(-gate)))


def step_kernel(
    kv, tp,
    tok, wq, wk, wv, wz, wo, state, gain_in, ws_in, wd_in, rate_in, extra_in, strength_in,
    decay_in, accepted_in, parent_in, old_in, ov_in, hgain_in, ogain_in,
    out_ref, st,
    xt, wt, gcol, wqk, wout, wx, wxt, ok, kt, natural, turned, sc, vz, m, sq, squares, xb, parts,
    mine, sums,
    gain, ws, wd, rate, extra, strength, decay, accepted, parent, old, ov, hgain, ogain,
    local, tsem, ssem, send, recv, both, wsend, wrecv, qsend, qrecv, send2, recv2, both2,
    psend, precv, esend, erecv,
):
    grid = Grid(kv, tp)
    grid.here()
    prop, own, seqs = tok.shape
    width, cols = wq.shape
    small = wv.shape[0]
    heads, vdim, hd = st.shape[1:]
    part = wout.shape[1] // kv
    chips = kv * tp // 2
    tiles = seqs // LANES
    pairs = prop // 2
    units = tiles * pairs
    lane = lax.axis_index("tp")
    me = lax.axis_index("kv") * tp + lane
    mine_kv = grid.group((0, 0, 0))
    far = grid.device((0, 0, 0), 1)

    def piece_of(u, half):
        return (u % pairs) * 2 + half, slice((u // pairs) * LANES, (u // pairs + 1) * LANES)

    here = (grid.chip((0, 0, 0)), grid.core)
    token_loads = {}
    for u in range(units):
        for half in range(2):
            p, span = piece_of(u, half)
            token_loads[u, half] = pltpu.make_async_copy(
                tok.at[p, :, span],
                xt.at[u, here[0], here[1], :, pl.ds(half * LANES, LANES)],
                tsem.at[u, half],
            )
            token_loads[u, half].start()
    loads = [
        pltpu.make_async_copy(wo, wout, local.at[0]),
        pltpu.make_async_copy(wq, wqk.at[0], local.at[1]),
        pltpu.make_async_copy(wk, wqk.at[1], local.at[2]),
        pltpu.make_async_copy(wv, wt.at[pl.ds(2 * cols, small)], local.at[3]),
        pltpu.make_async_copy(wz, wt.at[pl.ds(2 * cols + small, small)], local.at[4]),
    ]
    little = zip(
        (gain_in, ws_in, wd_in, rate_in, extra_in, strength_in, decay_in, accepted_in, parent_in,
         old_in, ov_in, hgain_in, ogain_in),
        (gain, ws, wd, rate, extra, strength, decay, accepted, parent, old, ov, hgain, ogain),
    )
    for index, (source, target) in enumerate(little):
        loads.append(pltpu.make_async_copy(source, target, local.at[5 + index]))
    for load in loads:
        load.start()
    state_loads = {}
    for t in range(tiles):
        for h in range(heads):
            state_loads[t, h] = pltpu.make_async_copy(
                state.at[pl.ds(t * LANES, LANES), h], st.at[pl.ds(t * LANES, LANES), h],
                ssem.at[t, h],
            )
            state_loads[t, h].start()

    everyone = [(o, f) for o in offsets(grid.sizes) for f in (0, 1)]
    everyone = [e for e in everyone if any(e[0]) or e[1]]
    row = [(o, f) for o, f in everyone if not o[0] and not o[1]]
    plane = [o for o in offsets((grid.z, grid.y, 1)) if any(o)]
    line = [(0, 0, c) for c in range(1, grid.x)]
    meet(grid, everyone)

    tokens = Spread(
        grid, grid.sizes, ORDERS,
        lambda u, half, offset, core: xt.at[
            u, grid.chip(offset), core, :, pl.ds(half * LANES, LANES)
        ],
        send, recv, both,
    )
    blend = Spread(
        grid, (grid.z, grid.y, 1), FLAT,
        lambda u, half, offset, core: xb.at[u, grid.group(offset), core],
        send2, recv2, both2,
    )

    def weights_in():
        for load in loads:
            load.wait()
        gains = gain[...].astype(f32)
        for first in range(0, width, 128):
            piece = gains[first // 128 : first // 128 + 1, :]
            gcol[first : first + 128, :] = jnp.broadcast_to(piece, (128, 128)).T
        for which in range(2):
            for first in range(0, width, 256):
                piece = wqk[which, first : first + 256, :].astype(f32)
                wt[which * cols : (which + 1) * cols, first : first + 256] = piece.T.astype(bf16)
        tail = wt.shape[0] - 2 * cols - 2 * small
        rows = [ws[...].astype(f32), wd[...].astype(f32)]
        rows.append(jnp.zeros((tail - 2 * heads, width), f32))
        wt[2 * cols + 2 * small :, :] = jnp.concatenate(rows, axis=0).astype(bf16)
        for p in range(prop):
            ok[p] = old[:, p, :]

    def take_up(t, h):
        state_loads[t, h].wait()
        advance(st, ok, kt, ov, strength, decay, accepted, t, h)

    def weights_out():
        for index, offset in enumerate(plane):
            start = pl.multiple_of(grid.group(offset) * part, part)
            remote(
                wout.at[:, pl.ds(start, part)], wx.at[mine_kv, grid.core],
                wsend.at[0], wrecv.at[index], grid.device(offset),
            ).start()
        wx[mine_kv, grid.core] = wout[:, pl.ds(pl.multiple_of(mine_kv * part, part), part)]
        remote(
            wout.at[:, pl.ds(pl.multiple_of(mine_kv * part, part), part)],
            wx.at[mine_kv, grid.core], wsend.at[1], wrecv.at[len(plane)], far,
        ).start()

    def weights_over():
        for index, offset in enumerate(plane):
            view = wx.at[grid.group(negated(offset, grid.sizes)), grid.core]
            remote(view, view, wsend.at[0], wrecv.at[index], far).wait_recv()
            remote(view, view, wsend.at[1], wrecv.at[len(plane)], far).start()

    def weights_turn():
        other = wx.at[:, 1 - grid.core]
        remote(other, other, wsend.at[1], wrecv.at[len(plane)], far).wait_recv()
        for g in range(kv):
            piece = wx[g].reshape(2 * small, part).astype(f32)
            wxt[g] = piece.T.astype(bf16)

    def finish(u):
        tokens.shared(u, xt.at[u, :, 1 - grid.core])
        x = xt[u].reshape(width, 2 * LANES).astype(f32)
        square = jnp.sum(x * x, axis=0, keepdims=True)
        scale = lax.rsqrt(square / width + epsilon)
        g = jnp.concatenate([gcol[...]] * 2, axis=1)
        normed = (x * scale * g).astype(bf16)
        out = jnp.dot(wt[...], normed, preferred_element_type=f32)
        for half in range(2):
            p, span = piece_of(u, half)
            lanes = slice(half * LANES, (half + 1) * LANES)
            for which in range(2):
                block = out[which * cols : (which + 1) * cols, lanes].astype(bf16).astype(f32)
                turned[which, p, :, span] = block
                natural[which, p, span, :] = block.T.astype(bf16)
                first = 2 * cols + which * small
                vz[which, p, :, span] = out[first : first + small, lanes].astype(bf16)
            side = out[2 * cols + 2 * small :, lanes]
            for h in range(heads):
                pre = side[heads + h : heads + h + 1]
                beta = 1.0 / (1.0 + jnp.exp(-side[h : h + 1]))
                soft = jnp.maximum(pre, 0.0) + jnp.log1p(jnp.exp(-jnp.abs(pre)))
                g_new = -rate[0:1, h : h + 1] * soft + extra[p, h : h + 1, span]
                sc[p, h, 0:1, span] = beta
                sc[p, h, 1:2, span] = g_new
                sc[p, h, 2:3, span] = parent[p : p + 1, span].astype(f32)

    def read_out(t):
        gains = column(hgain[...])
        for h in range(heads):
            propose(st, natural, turned, sc, vz, gains, m, sq, t, h)
        for index, (offset, flip) in enumerate(row):
            remote(
                sq.at[t], squares.at[t, lane], qsend.at[t, index], qrecv.at[t, index],
                grid.device(offset, flip),
            ).start()
        squares[t, lane] = sq[t]

    def blend_out(t):
        for index, (offset, flip) in enumerate(row):
            remote(
                sq.at[t], squares.at[t, lane], qsend.at[t, index], qrecv.at[t, index],
                grid.device(offset, flip),
            ).wait()
        everything = total([squares[t, i] for i in range(tp)])
        scale = lax.rsqrt(everything / hd + epsilon)
        for u in range(t * pairs, (t + 1) * pairs):
            for half in range(2):
                p, span = piece_of(u, half)
                scaled = [
                    m[p, h * vdim : (h + 1) * vdim, span]
                    * scale[h * prop + p : h * prop + p + 1, :]
                    for h in range(heads)
                ]
                xb[u, mine_kv, grid.core, :, half * LANES : (half + 1) * LANES] = (
                    jnp.concatenate(scaled, axis=0).astype(bf16)
                )
            blend.begin(u)

    def exchange(u, index, offset):
        target = grid.shift(offset)[2] * 2 + grid.core
        return remote(
            parts.at[u, target], mine.at[u, index], psend.at[u, index], precv.at[u, index],
            grid.device(offset),
        )

    def multiply(u):
        blend.shared(u, xb.at[u, :, 1 - grid.core])
        out = None
        for g in range(kv):
            term = jnp.dot(
                wxt[g], xb[u, g].reshape(2 * small, 2 * LANES), preferred_element_type=f32
            )
            out = term if out is None else out + term
        parts[u] = out.reshape(part // own, own, 2 * LANES)
        for index, offset in enumerate(line):
            exchange(u, index, offset).start()

    slot = grid.at[2] * 2 + grid.core

    def square_out(t):
        for u in range(t * pairs, (t + 1) * pairs):
            acc = parts[u, slot]
            for index, offset in enumerate(line):
                exchange(u, index, offset).wait()
                acc = acc + mine[u, index]
            parts[u, slot] = acc
            pp = u - t * pairs
            sums[t, me, pp : pp + 1, :] = jnp.sum(acc * acc, axis=0, keepdims=True)
        for index, (offset, flip) in enumerate(everyone):
            remote(
                sums.at[t, me], sums.at[t, me], esend.at[t], erecv.at[t, index],
                grid.device(offset, flip),
            ).start()

    def end(t):
        for index, (offset, flip) in enumerate(everyone):
            kv_from, tp_from = grid.device(negated(offset, grid.sizes), flip)
            view = sums.at[t, kv_from * tp + tp_from]
            remote(view, view, esend.at[t], erecv.at[t, index], far).wait_recv()
        final = lax.rsqrt(jnp.sum(sums[t], axis=0) / width + epsilon)
        g = column(ogain[...])
        for u in range(t * pairs, (t + 1) * pairs):
            pp = u - t * pairs
            for half in range(2):
                p, span = piece_of(u, half)
                lanes = slice(half * LANES, (half + 1) * LANES)
                out_ref[p, :, span] = (
                    parts[u, slot][:, lanes] * final[pp : pp + 1, lanes] * g
                ).astype(bf16)

    for u in range(units):
        for half in range(2):
            token_loads[u, half].wait()
        tokens.begin(u)

    tasks = [(0.5, weights_in), (2.7, weights_out), (WEIGHTS_OVER, weights_over)]
    for u in range(units):
        for level in (1, 2, 3):
            tasks.append((level + 0.5 * u, functools.partial(tokens.level, u, level)))
        tasks.append((3.001 + 0.5 * u, functools.partial(finish, u)))
    places = [(t, h) for t in range(tiles) for h in range(heads)]
    for index, (t, h) in enumerate(places):
        tasks.append((TAKE_UP + 0.4 * index * 4 / len(places), functools.partial(take_up, t, h)))
    last = 3.0 + 0.5 * (units - 1)
    tasks.append((last + 0.02, weights_turn))
    for t in range(tiles):
        ready = 3.0 + 0.5 * ((t + 1) * pairs - 1)
        tasks.append((ready + 0.01, functools.partial(read_out, t)))
        sends = ready + 0.5005 if t < tiles - 1 else last + 0.03
        tasks.append((sends, functools.partial(blend_out, t)))
        for u in range(t * pairs, (t + 1) * pairs):
            first = last + 0.021 + 0.1 * t
            late = last + 0.04 + 0.1 * t
            tasks.append((first + 0.0001 * u, functools.partial(blend.level, u, 1)))
            tasks.append((late + 0.002 * u, functools.partial(blend.level, u, 2)))
            tasks.append((late + 0.002 * u + 0.001, functools.partial(multiply, u)))
        tasks.append((last + 0.13 + 0.1 * t, functools.partial(square_out, t)))
        tasks.append((last + 1.0 + t, functools.partial(end, t)))
    for _, task in sorted(tasks, key=lambda entry: entry[0]):
        task()

    rest = wx.at[pl.ds(0, kv - 1), 0]
    remote(rest, rest, wsend.at[0], wrecv.at[0], far).wait_send()
    whole = wx.at[:, 0]
    remote(whole, whole, wsend.at[1], wrecv.at[0], far).wait_send()
    for u in range(units):
        tokens.sent(u, xt.at[u, :, 0], xt.at[u, pl.ds(0, chips - 1), 0])
        blend.sent(u, xb.at[u, :, 0], xb.at[u, pl.ds(0, kv - 1), 0])
    for t in range(tiles):
        rest = sums.at[t, pl.ds(0, kv * tp - 1)]
        remote(rest, rest, esend.at[t], erecv.at[t, 0], far).wait_send()


WEIGHTS_OVER = 3.52
TAKE_UP = 1.6


def step(kv, tp, *args):
    tokens, wq, _, wv, _, wo, state = args[:7]
    prop, own, seqs = tokens.shape
    width, cols = wq.shape
    small = wv.shape[0]
    heads, vdim, hd = state.shape[1:]
    chips = kv * tp // 2
    part = wo.shape[1] // kv
    rows = 2 * cols + 2 * small + 16 * -(-2 * heads // 16)
    tiles = seqs // LANES
    units = tiles * (prop // 2)
    others = max(tp // 2 - 1, 1)
    vmem, dma = pltpu.VMEM, pltpu.SemaphoreType.DMA
    return pl.pallas_call(
        functools.partial(step_kernel, kv, tp),
        in_specs=[pl.BlockSpec(memory_space=pl.ANY)] * len(args),
        out_specs=[pl.BlockSpec(memory_space=pltpu.VMEM)] * 2,
        out_shape=[vmem((prop, own, seqs), bf16), vmem(state.shape, f32)],
        scratch_shapes=[
            vmem((units, chips, 2, own, 2 * LANES), bf16),
            vmem((rows, width), bf16),
            vmem((width, 128), f32),
            vmem((2, width, cols), bf16),
            vmem(wo.shape, bf16),
            vmem((kv, 2, small, part), bf16),
            vmem((kv, part, 2 * small), bf16),
            vmem((prop, seqs, cols), bf16),
            vmem((prop, hd, LANES), f32),
            vmem((2, prop, seqs, cols), bf16),
            vmem((2, prop, cols, seqs), f32),
            vmem((prop, heads, 8, seqs), f32),
            vmem((2, prop, small, seqs), bf16),
            vmem((prop, small, seqs), f32),
            vmem((tiles, heads * prop, LANES), f32),
            vmem((tiles, tp, heads * prop, LANES), f32),
            vmem((units, kv, 2, small, 2 * LANES), bf16),
            vmem((units, part // own, own, 2 * LANES), f32),
            vmem((units, others, own, 2 * LANES), f32),
            vmem((tiles, kv * tp, prop // 2, 2 * LANES), f32),
        ]
        + [vmem(x.shape, x.dtype) for x in args[7:]]
        + [
            dma((len(args) - 2,)),
            dma((units, 2)),
            dma((tiles, heads)),
            dma((units,)),
            dma((units, 2, chips)),
            dma((2, units)),
            dma((2,)),
            dma((kv,)),
            dma((tiles, tp)),
            dma((tiles, tp)),
            dma((units,)),
            dma((units, 1, kv)),
            dma((2, units)),
            dma((units, others)),
            dma((units, others)),
            dma((tiles,)),
            dma((tiles, kv * tp)),
        ],
        compiler_params=pltpu.CompilerParams(
            collective_id=0, has_side_effects=True, vmem_limit_bytes=VMEM_ALL - (9 << 20)
        ),
        cost_estimate=pl.CostEstimate(
            flops=2 * rows * width * prop * seqs, bytes_accessed=16 << 20, transcendentals=0
        ),
    )(*[x if x.size == 1 else pltpu.with_memory_space_constraint(x, pltpu.HBM) for x in args])


def on_device(
    kv,
    tp,
    tokens,
    input_norm_gain,
    query_weight,
    key_weight,
    value_weight,
    output_gate_weight,
    strength_weight,
    decay_weight,
    head_decay_rate,
    proposal_log_decay,
    head_norm_gain,
    output_weight,
    output_norm_gain,
    state,
    previous_keys,
    previous_values,
    previous_log_decay,
    previous_strengths,
    accepted,
    parent,
):
    seqs, heads, vdim, hd = state.shape
    prop = parent.shape[1]
    width = input_norm_gain.shape[0]
    channels = heads * vdim

    def turn(x):
        return jnp.transpose(x, (1, 2, 0))

    layer_out, accepted_state = step(
        kv, tp,
        turn(tokens),
        query_weight,
        key_weight,
        turn(value_weight).reshape(channels, width),
        turn(output_gate_weight).reshape(channels, width),
        output_weight.reshape(channels, width),
        state,
        input_norm_gain.reshape(width // 128, 128),
        strength_weight.T,
        decay_weight.T,
        head_decay_rate[None, :],
        turn(proposal_log_decay),
        turn(previous_strengths),
        turn(previous_log_decay),
        accepted[None, :],
        parent.T,
        previous_keys,
        jnp.transpose(previous_values, (1, 2, 3, 0)).reshape(prop, channels, seqs),
        head_norm_gain[None, :],
        output_norm_gain[None, :],
    )
    return (jnp.transpose(layer_out, (2, 0, 1)), accepted_state)


def solution(mesh):
    placed = (
        P(None, None, AXES),
        P(),
        P(None, "kv"),
        P(None, "kv"),
        P(None, "kv", "tp"),
        P(None, "kv", "tp"),
        P(None, "kv"),
        P(None, "kv"),
        P("kv"),
        P(None, None, "kv"),
        P("tp"),
        P("kv", "tp", None),
        P(AXES),
        P(None, "kv", "tp", None),
        P(None, None, "kv"),
        P(None, None, "kv", "tp"),
        P(None, None, "kv"),
        P(None, None, "kv"),
        P(),
        P(),
    )
    return jax.shard_map(
        functools.partial(on_device, mesh.shape["kv"], mesh.shape["tp"]),
        mesh=mesh,
        in_specs=placed,
        out_specs=(P(None, None, AXES), P(None, "kv", "tp", None)),
        check_vma=False,
    )
```

```python
import functools

import jax
import jax.numpy as jnp
from jax import lax
from jax.experimental import pallas as pl
from jax.experimental.pallas import tpu as pltpu
from jax.sharding import PartitionSpec as P

epsilon = 1e-06
GROUP = 16
AXES = ("kv", "tp")
MESH = pl.DeviceIdType.MESH
f32, bf16 = jnp.float32, jnp.bfloat16


class Grid:
    def __init__(self, kv, tp):
        self.kv, self.tp = kv, tp
        self.x = tp // 2
        self.y = self.x if kv % self.x == 0 else 1
        self.z = kv // self.y
        self.sizes = (self.z, self.y, self.x)

    def here(self):
        kv, tp = lax.axis_index("kv"), lax.axis_index("tp")
        self.at = (kv // self.y, lax.rem(kv, self.y), tp // 2)
        self.core = lax.rem(tp, 2)

    def shift(self, offset):
        return tuple(lax.rem(a + o % n, n) for a, o, n in zip(self.at, offset, self.sizes))

    def device(self, offset, flip=0):
        z, y, x = self.shift(offset)
        core = 1 - self.core if flip else self.core
        return (z * self.y + y, x * 2 + core)

    def chip(self, offset):
        z, y, x = self.shift(offset)
        return (z * self.y + y) * self.x + x

    def group(self, offset):
        z, y, _ = self.shift(offset)
        return z * self.y + y


def offsets(sizes):
    return [(a, b, c) for a in range(sizes[0]) for b in range(sizes[1]) for c in range(sizes[2])]


def negated(offset, sizes):
    return tuple(-o % n for o, n in zip(offset, sizes))


def meet(grid, peers):
    barrier = pltpu.get_barrier_semaphore()
    for offset, flip in peers:
        pl.semaphore_signal(
            barrier, inc=1, device_id=grid.device(offset, flip), device_id_type=MESH
        )
    pl.semaphore_wait(barrier, len(peers))


def remote(src, dst, send, recv, device):
    return pltpu.make_async_remote_copy(
        src_ref=src, dst_ref=dst, send_sem=send, recv_sem=recv, device_id=device,
        device_id_type=MESH,
    )


def tree(sizes, order):
    steps = []
    for offset in offsets(sizes):
        reached = max([order.index(d) + 1 for d in range(3) if offset[d]], default=0)
        onward = [(d, k) for d in order[reached:] for k in range(1, sizes[d])]
        steps.append((offset, onward))
    return steps


def unit(dim, sign):
    return tuple(sign if d == dim else 0 for d in range(3))


class Spread:
    def __init__(self, grid, sizes, orders, place, send, recv, both):
        self.grid, self.sizes, self.orders = grid, sizes, orders
        self.place, self.send, self.recv, self.both = place, send, recv, both

    def slot(self, offset):
        a, b, c = offset
        return (a * self.sizes[1] + b) * self.sizes[2] + c

    def view(self, u, half, offset):
        sign = self.orders[half][1]
        return self.place(u, half, tuple(-sign * o for o in offset), self.grid.core)

    def pass_on(self, u, half, offset, onward):
        sign = self.orders[half][1]
        here = self.view(u, half, offset)
        for dim, count in onward:
            landed = tuple(o + (count if d == dim else 0) for d, o in enumerate(offset))
            remote(
                here, here, self.send.at[u], self.recv.at[u, half, self.slot(landed)],
                self.grid.device(unit(dim, sign * count)),
            ).start()
        remote(
            here, here, self.both.at[0, u], self.both.at[1, u], self.grid.device((0, 0, 0), 1)
        ).start()

    def begin(self, u):
        for half, (order, _) in enumerate(self.orders):
            for offset, onward in tree(self.sizes, order):
                if not any(offset):
                    self.pass_on(u, half, offset, onward)

    def level(self, u, wanted):
        for half, (order, _) in enumerate(self.orders):
            for offset, onward in tree(self.sizes, order):
                if sum(1 for o in offset if o) != wanted:
                    continue
                here = self.view(u, half, offset)
                remote(
                    here, here, self.send.at[u], self.recv.at[u, half, self.slot(offset)],
                    self.grid.device((0, 0, 0), 1),
                ).wait_recv()
                self.pass_on(u, half, offset, onward)

    def shared(self, u, whole):
        remote(whole, whole, self.both.at[0, u], self.both.at[1, u],
               self.grid.device((0, 0, 0), 1)).wait_recv()

    def sent(self, u, whole, rest):
        far = self.grid.device((0, 0, 0), 1)
        remote(rest, rest, self.send.at[u], self.both.at[1, u], far).wait_send()
        remote(whole, whole, self.both.at[0, u], self.both.at[1, u], far).wait_send()


ORDERS = (((0, 1, 2), 1), ((0, 2, 1), -1))
FLAT = (((0, 1, 2), 1),)
VMEM_ALL = 67043328
LANES = 128


def column(row):
    size = row.shape[1]
    square = (size, size)
    chosen = lax.broadcasted_iota(jnp.int32, square, 0) == lax.broadcasted_iota(jnp.int32, square, 1)
    wide = jnp.broadcast_to(row.astype(f32), square)
    return jnp.sum(jnp.where(chosen, wide, 0.0), axis=1, keepdims=True)


def total(terms):
    terms = list(terms)
    while len(terms) > 1:
        terms = [sum(terms[i : i + 2][1:], terms[i]) for i in range(0, len(terms), 2)]
    return terms[0]


def swap(outer, groups, source, sources, targets):
    shifted = []
    for d in range(groups):
        acc = None
        for a in range(sources):
            t = (a - d) % groups
            if t >= targets:
                continue
            acc = source[a] if acc is None else jnp.where(outer == t, source[a], acc)
        shifted.append(acc if acc is None or d == 0 else pltpu.roll(acc, d * GROUP, 1))
    results = []
    for t in range(targets):
        acc = None
        for a in range(sources):
            piece = shifted[(a - t) % groups]
            acc = piece if acc is None else jnp.where(outer == a, piece, acc)
        results.append(acc)
    return results


def read_state(st, start, h, tiles_of, count):
    vdim, hd = st.shape[2], st.shape[3]
    groups = LANES // GROUP
    lane = lax.broadcasted_iota(jnp.int32, (vdim, LANES), 1)
    inner, outer = lane % GROUP, lane // GROUP
    products = []
    for c in range(groups):
        first = start + c * GROUP
        rows = st[first : first + GROUP, h].reshape(GROUP * vdim, hd).astype(bf16)
        keys = jnp.concatenate(tiles_of(first), axis=0)
        product = lax.dot_general(
            rows, keys, (((1,), (1,)), ((), ())), preferred_element_type=f32
        )
        width = count * GROUP
        chosen = product[:vdim]
        for s in range(1, GROUP):
            chosen = jnp.where(
                inner[:, :width] == s, product[s * vdim : (s + 1) * vdim], chosen
            )
        if width < LANES:
            chosen = jnp.concatenate([chosen, jnp.zeros((vdim, LANES - width), f32)], axis=1)
        products.append(chosen)
    return swap(outer, groups, products, groups, count)


def advance(st, ok, kt, ov, strength, decay, accepted, t, h):
    prop, _, _ = ok.shape
    vdim, hd = st.shape[2], st.shape[3]
    start = t * LANES
    span = slice(start, start + LANES)
    cols = slice(h * hd, (h + 1) * hd)
    groups = LANES // GROUP
    for p in range(prop):
        kt[p] = ok[p, span, cols].astype(f32).T
    inv = [lax.rsqrt(jnp.sum(kt[p] * kt[p], axis=0, keepdims=True) + epsilon) for p in range(prop)]
    count = accepted[:, span]
    live = [jnp.where(count > p, 1.0, 0.0) for p in range(prop)]
    beta = [strength[p, h : h + 1, span] * live[p] for p in range(prop)]
    gam = []
    for p in range(prop):
        step = decay[p, h : h + 1, span] * live[p]
        gam.append(step if p == 0 else gam[-1] + step)
    raw = read_state(
        st, start, h, lambda first: [ok[p, first : first + GROUP, cols] for p in range(prop)], prop
    )
    update = []
    for i in range(prop):
        value = ov[i, h * vdim : (h + 1) * vdim, span].astype(f32)
        acc = beta[i] * value - (beta[i] * jnp.exp(gam[i]) * inv[i]) * raw[i]
        for j in range(i):
            gram = jnp.sum(kt[i] * kt[j], axis=0, keepdims=True) * (inv[i] * inv[j])
            acc = acc - (beta[i] * gram * jnp.exp(jnp.minimum(gam[i] - gam[j], 0.0))) * update[j]
        update.append(acc)
    weighted = [update[j] * (jnp.exp(gam[-1] - gam[j]) * inv[j]) for j in range(prop)]
    lane = lax.broadcasted_iota(jnp.int32, (vdim, LANES), 1)
    inner, outer = lane % GROUP, lane // GROUP
    compact = swap(outer, groups, weighted, prop, groups)
    width = prop * GROUP
    narrow = inner[:, :width]
    fade = jnp.broadcast_to(jnp.exp(gam[-1]), (LANES, LANES)).T
    for c in range(groups):
        first = start + c * GROUP
        keys = jnp.concatenate([ok[p, first : first + GROUP, cols] for p in range(prop)], axis=0)
        piece = compact[c][:, :width]
        left = jnp.concatenate(
            [jnp.where(narrow == s, piece, 0.0) for s in range(GROUP)], axis=0
        ).astype(bf16)
        delta = jnp.dot(left, keys, preferred_element_type=f32)
        for s in range(GROUP):
            seq = c * GROUP + s
            st[start + seq, h] = (
                st[start + seq, h] * fade[seq : seq + 1, :hd] + delta[s * vdim : (s + 1) * vdim]
            )


def propose(st, natural, turned, sc, vz, hgain, m, sq, t, h):
    prop = natural.shape[1]
    vdim, hd = st.shape[2], st.shape[3]
    start = t * LANES
    span = slice(start, start + LANES)
    cols = slice(h * hd, (h + 1) * hd)
    vrows = slice(h * vdim, (h + 1) * vdim)

    def vector(which, p):
        return turned[which, p, cols, span]

    def dot(a, b):
        return jnp.sum(vector(*a) * vector(*b), axis=0, keepdims=True)

    inv_q = [
        lax.rsqrt(dot((0, p), (0, p)) + epsilon) * hd ** (-0.5) for p in range(prop)
    ]
    inv = [lax.rsqrt(dot((1, p), (1, p)) + epsilon) for p in range(prop)]
    beta = [sc[p, h, 0:1, span] for p in range(prop)]
    g = [sc[p, h, 1:2, span] for p in range(prop)]
    parents = [sc[p, h, 2:3, span] for p in range(prop)]
    ancestor = []
    for i in range(prop):
        direct = [jnp.where(parents[i] == float(j), 1.0, 0.0) for j in range(i)]
        row = []
        for j in range(i):
            row.append(total([direct[j]] + [direct[k] * ancestor[k][j] for k in range(j + 1, i)]))
        ancestor.append(row)
    gam = []
    for i in range(prop):
        gam.append(total([g[i]] + [ancestor[i][j] * g[j] for j in range(i)]))
    dec = {
        (i, j): jnp.exp(jnp.minimum(gam[i] - gam[j], 0.0)) * ancestor[i][j]
        for i in range(prop)
        for j in range(i)
    }
    raw = read_state(
        st, start, h,
        lambda first: [
            natural[which, p, first : first + GROUP, cols] for which in (1, 0) for p in range(prop)
        ],
        2 * prop,
    )
    update = []
    for i in range(prop):
        value = vz[0, i, vrows, span].astype(f32)
        acc = beta[i] * value - (beta[i] * jnp.exp(gam[i]) * inv[i]) * raw[i]
        for j in range(i):
            gram = dot((1, i), (1, j)) * (inv[i] * inv[j])
            acc = acc - (beta[i] * gram * dec[i, j]) * update[j]
        update.append(acc)
    for p in range(prop):
        acc = (jnp.exp(gam[p]) * inv_q[p]) * raw[prop + p]
        for j in range(p + 1):
            weight = dot((0, p), (1, j)) * (inv_q[p] * inv[j])
            acc = acc + (weight if j == p else weight * dec[p, j]) * update[j]
        sq[t, h * prop + p : h * prop + p + 1, :] = jnp.sum(acc * acc, axis=0, keepdims=True)
        gate = vz[1, p, vrows, span].astype(f32)
        m[p, vrows, span] = acc * hgain * (gate / (1.0 + jnp.exp(-gate)))


def step_kernel(
    kv, tp,
    tok, wq, wk, wv, wz, wo, state, gain_in, ws_in, wd_in, rate_in, extra_in, strength_in,
    decay_in, accepted_in, parent_in, old_in, ov_in, hgain_in, ogain_in,
    out_ref, st,
    xt, wt, gcol, wqk, wout, wx, wxt, ok, kt, natural, turned, sc, vz, m, sq, squares, xb, parts,
    leave, mine, sums,
    gain, ws, wd, rate, extra, strength, decay, accepted, parent, old, ov, hgain, ogain,
    local, tsem, ssem, send, recv, both, wsend, wrecv, qsend, qrecv, send2, recv2, both2,
    psend, precv, esend, erecv,
):
    grid = Grid(kv, tp)
    grid.here()
    prop, own, seqs = tok.shape
    width, cols = wq.shape
    small = wv.shape[0]
    heads, vdim, hd = st.shape[1:]
    part = wout.shape[1] // kv
    chips = kv * tp // 2
    tiles = seqs // LANES
    pairs = prop // 2
    units = tiles * pairs
    lane = lax.axis_index("tp")
    me = lax.axis_index("kv") * tp + lane
    mine_kv = grid.group((0, 0, 0))
    far = grid.device((0, 0, 0), 1)

    def piece_of(u, half):
        return (u % pairs) * 2 + half, slice((u // pairs) * LANES, (u // pairs + 1) * LANES)

    here = (grid.chip((0, 0, 0)), grid.core)
    token_loads = {}
    for u in range(units):
        for half in range(2):
            p, span = piece_of(u, half)
            token_loads[u, half] = pltpu.make_async_copy(
                tok.at[p, :, span],
                xt.at[u, here[0], here[1], :, pl.ds(half * LANES, LANES)],
                tsem.at[u, half],
            )
            token_loads[u, half].start()
    loads = [
        pltpu.make_async_copy(wo, wout, local.at[0]),
        pltpu.make_async_copy(wq, wqk.at[0], local.at[1]),
        pltpu.make_async_copy(wk, wqk.at[1], local.at[2]),
        pltpu.make_async_copy(wv, wt.at[pl.ds(2 * cols, small)], local.at[3]),
        pltpu.make_async_copy(wz, wt.at[pl.ds(2 * cols + small, small)], local.at[4]),
    ]
    little = zip(
        (gain_in, ws_in, wd_in, rate_in, extra_in, strength_in, decay_in, accepted_in, parent_in,
         old_in, ov_in, hgain_in, ogain_in),
        (gain, ws, wd, rate, extra, strength, decay, accepted, parent, old, ov, hgain, ogain),
    )
    for index, (source, target) in enumerate(little):
        loads.append(pltpu.make_async_copy(source, target, local.at[5 + index]))
    for load in loads:
        load.start()
    state_loads = {}
    for t in range(tiles):
        for h in range(heads):
            state_loads[t, h] = pltpu.make_async_copy(
                state.at[pl.ds(t * LANES, LANES), h], st.at[pl.ds(t * LANES, LANES), h],
                ssem.at[t, h],
            )
            state_loads[t, h].start()

    everyone = [(o, f) for o in offsets(grid.sizes) for f in (0, 1)]
    everyone = [e for e in everyone if any(e[0]) or e[1]]
    row = [(o, f) for o, f in everyone if not o[0] and not o[1]]
    plane = [o for o in offsets((grid.z, grid.y, 1)) if any(o)]
    line = [(0, 0, c) for c in range(1, grid.x)]
    near = [(unit(d, k), 0) for d in range(3) for k in range(1, grid.sizes[d])]
    meet(grid, near + [((0, 0, 0), 1)])

    tokens = Spread(
        grid, grid.sizes, ORDERS,
        lambda u, half, offset, core: xt.at[
            u, grid.chip(offset), core, :, pl.ds(half * LANES, LANES)
        ],
        send, recv, both,
    )
    blend = Spread(
        grid, (grid.z, grid.y, 1), FLAT,
        lambda u, half, offset, core: xb.at[u, grid.group(offset), core],
        send2, recv2, both2,
    )

    def weights_in():
        for load in loads:
            load.wait()
        gains = gain[...].astype(f32)
        for first in range(0, width, 128):
            piece = gains[first // 128 : first // 128 + 1, :]
            gcol[first : first + 128, :] = jnp.broadcast_to(piece, (128, 128)).T
        for which in range(2):
            for first in range(0, width, 256):
                piece = wqk[which, first : first + 256, :].astype(f32)
                wt[which * cols : (which + 1) * cols, first : first + 256] = piece.T.astype(bf16)
        tail = wt.shape[0] - 2 * cols - 2 * small
        rows = [ws[...].astype(f32), wd[...].astype(f32)]
        rows.append(jnp.zeros((tail - 2 * heads, width), f32))
        wt[2 * cols + 2 * small :, :] = jnp.concatenate(rows, axis=0).astype(bf16)
        for p in range(prop):
            ok[p] = old[:, p, :]

    def take_up(t, h):
        state_loads[t, h].wait()
        advance(st, ok, kt, ov, strength, decay, accepted, t, h)

    def weights_out():
        for index, offset in enumerate(plane):
            start = pl.multiple_of(grid.group(offset) * part, part)
            remote(
                wout.at[:, pl.ds(start, part)], wx.at[mine_kv, grid.core],
                wsend.at[0], wrecv.at[index], grid.device(offset),
            ).start()
        wx[mine_kv, grid.core] = wout[:, pl.ds(pl.multiple_of(mine_kv * part, part), part)]
        remote(
            wout.at[:, pl.ds(pl.multiple_of(mine_kv * part, part), part)],
            wx.at[mine_kv, grid.core], wsend.at[1], wrecv.at[len(plane)], far,
        ).start()

    def weights_over():
        for index, offset in enumerate(plane):
            view = wx.at[grid.group(negated(offset, grid.sizes)), grid.core]
            remote(view, view, wsend.at[0], wrecv.at[index], far).wait_recv()
            remote(view, view, wsend.at[1], wrecv.at[len(plane)], far).start()

    def weights_turn():
        other = wx.at[:, 1 - grid.core]
        remote(other, other, wsend.at[1], wrecv.at[len(plane)], far).wait_recv()
        for g in range(kv):
            piece = wx[g].reshape(2 * small, part).astype(f32)
            wxt[g] = piece.T.astype(bf16)

    def finish(u):
        tokens.shared(u, xt.at[u, :, 1 - grid.core])
        x = xt[u].reshape(width, 2 * LANES).astype(f32)
        square = jnp.sum(x * x, axis=0, keepdims=True)
        scale = lax.rsqrt(square / width + epsilon)
        g = jnp.concatenate([gcol[...]] * 2, axis=1)
        normed = (x * scale * g).astype(bf16)
        out = jnp.dot(wt[...], normed, preferred_element_type=f32)
        for half in range(2):
            p, span = piece_of(u, half)
            lanes = slice(half * LANES, (half + 1) * LANES)
            for which in range(2):
                block = out[which * cols : (which + 1) * cols, lanes].astype(bf16).astype(f32)
                turned[which, p, :, span] = block
                natural[which, p, span, :] = block.T.astype(bf16)
                first = 2 * cols + which * small
                vz[which, p, :, span] = out[first : first + small, lanes].astype(bf16)
            side = out[2 * cols + 2 * small :, lanes]
            for h in range(heads):
                pre = side[heads + h : heads + h + 1]
                beta = 1.0 / (1.0 + jnp.exp(-side[h : h + 1]))
                soft = jnp.maximum(pre, 0.0) + jnp.log1p(jnp.exp(-jnp.abs(pre)))
                g_new = -rate[0:1, h : h + 1] * soft + extra[p, h : h + 1, span]
                sc[p, h, 0:1, span] = beta
                sc[p, h, 1:2, span] = g_new
                sc[p, h, 2:3, span] = parent[p : p + 1, span].astype(f32)

    def read_out(t):
        gains = column(hgain[...])
        for h in range(heads):
            propose(st, natural, turned, sc, vz, gains, m, sq, t, h)
        for index, (offset, flip) in enumerate(row):
            remote(
                sq.at[t], squares.at[t, lane], qsend.at[t, index], qrecv.at[t, index],
                grid.device(offset, flip),
            ).start()
        squares[t, lane] = sq[t]

    def blend_out(t):
        for index, (offset, flip) in enumerate(row):
            remote(
                sq.at[t], squares.at[t, lane], qsend.at[t, index], qrecv.at[t, index],
                grid.device(offset, flip),
            ).wait()
        everything = total([squares[t, i] for i in range(tp)])
        scale = lax.rsqrt(everything / hd + epsilon)
        for u in range(t * pairs, (t + 1) * pairs):
            for half in range(2):
                p, span = piece_of(u, half)
                scaled = [
                    m[p, h * vdim : (h + 1) * vdim, span]
                    * scale[h * prop + p : h * prop + p + 1, :]
                    for h in range(heads)
                ]
                xb[u, mine_kv, grid.core, :, half * LANES : (half + 1) * LANES] = (
                    jnp.concatenate(scaled, axis=0).astype(bf16)
                )
            blend.begin(u)

    def exchange(u, index, offset):
        target = grid.shift(offset)[2] * 2 + grid.core
        return remote(
            leave.at[u, target], mine.at[u, index], psend.at[u, index], precv.at[u, index],
            grid.device(offset),
        )

    def multiply(u):
        blend.shared(u, xb.at[u, :, 1 - grid.core])
        out = None
        for g in range(kv):
            term = jnp.dot(
                wxt[g], xb[u, g].reshape(2 * small, 2 * LANES), preferred_element_type=f32
            )
            out = term if out is None else out + term
        parts[u] = out.reshape(part // own, own, 2 * LANES)
        leave[u] = parts[u].astype(bf16)
        for index, offset in enumerate(line):
            exchange(u, index, offset).start()

    slot = grid.at[2] * 2 + grid.core

    def square_out(t):
        for u in range(t * pairs, (t + 1) * pairs):
            acc = parts[u, slot]
            for index, offset in enumerate(line):
                exchange(u, index, offset).wait()
                acc = acc + mine[u, index].astype(f32)
            parts[u, slot] = acc
            pp = u - t * pairs
            sums[t, me, pp : pp + 1, :] = jnp.sum(acc * acc, axis=0, keepdims=True)
        for index, (offset, flip) in enumerate(everyone):
            remote(
                sums.at[t, me], sums.at[t, me], esend.at[t], erecv.at[t, index],
                grid.device(offset, flip),
            ).start()

    def end(t):
        for index, (offset, flip) in enumerate(everyone):
            kv_from, tp_from = grid.device(negated(offset, grid.sizes), flip)
            view = sums.at[t, kv_from * tp + tp_from]
            remote(view, view, esend.at[t], erecv.at[t, index], far).wait_recv()
        final = lax.rsqrt(jnp.sum(sums[t], axis=0) / width + epsilon)
        g = column(ogain[...])
        for u in range(t * pairs, (t + 1) * pairs):
            pp = u - t * pairs
            for half in range(2):
                p, span = piece_of(u, half)
                lanes = slice(half * LANES, (half + 1) * LANES)
                out_ref[p, :, span] = (
                    parts[u, slot][:, lanes] * final[pp : pp + 1, lanes] * g
                ).astype(bf16)

    for u in range(units):
        for half in range(2):
            token_loads[u, half].wait()
        tokens.begin(u)

    tasks = [(0.5, weights_in), (W_OUT, weights_out), (W_OVER, weights_over), (W_TURN, weights_turn)]
    places = [(t, h) for t in range(tiles) for h in range(heads)]
    for index, (t, h) in enumerate(places):
        tasks.append((TAKE_UP[min(index, len(TAKE_UP) - 1)], functools.partial(take_up, t, h)))
    for t in range(tiles):
        when = TIMES[min(t, 1)] + (t // 2,)
        lift = when[-1] * 10.0
        for pp in range(pairs):
            u = t * pairs + pp
            for level in (1, 2, 3):
                tasks.append((lift + when[0][level - 1][pp], functools.partial(tokens.level, u, level)))
            tasks.append((lift + when[0][2][pp] + 0.001, functools.partial(finish, u)))
            for level in (1, 2):
                tasks.append((lift + when[3][level - 1][pp], functools.partial(blend.level, u, level)))
            tasks.append((lift + when[3][1][pp] + 0.001, functools.partial(multiply, u)))
        tasks.append((lift + when[1], functools.partial(read_out, t)))
        tasks.append((lift + when[2], functools.partial(blend_out, t)))
        tasks.append((lift + when[4], functools.partial(square_out, t)))
        tasks.append((lift + when[5], functools.partial(end, t)))
    for _, task in sorted(tasks, key=lambda entry: entry[0]):
        task()

    rest = wx.at[pl.ds(0, kv - 1), 0]
    remote(rest, rest, wsend.at[0], wrecv.at[0], far).wait_send()
    whole = wx.at[:, 0]
    remote(whole, whole, wsend.at[1], wrecv.at[0], far).wait_send()
    for u in range(units):
        tokens.sent(u, xt.at[u, :, 0], xt.at[u, pl.ds(0, chips - 1), 0])
        blend.sent(u, xb.at[u, :, 0], xb.at[u, pl.ds(0, kv - 1), 0])
    for t in range(tiles):
        rest = sums.at[t, pl.ds(0, kv * tp - 1)]
        remote(rest, rest, esend.at[t], erecv.at[t, 0], far).wait_send()


TIMES = (
    (((1.0, 1.5), (2.0, 2.5), (3.0, 3.5)), 3.51, 4.0005, ((4.521, 4.522), (4.54, 4.542)), 4.63, 8.0),
    (((2.0, 2.5), (3.0, 3.5), (4.0, 4.5)), 4.51, 4.53, ((4.621, 4.622), (4.644, 4.646)), 4.73, 8.1),
)
TAKE_UP = (1.6, 2.01, 2.4, 2.8)
W_OUT, W_OVER, W_TURN = 3.002, 4.531, 4.5315


def step(kv, tp, *args):
    tokens, wq, _, wv, _, wo, state = args[:7]
    prop, own, seqs = tokens.shape
    width, cols = wq.shape
    small = wv.shape[0]
    heads, vdim, hd = state.shape[1:]
    chips = kv * tp // 2
    part = wo.shape[1] // kv
    rows = 2 * cols + 2 * small + 16 * -(-2 * heads // 16)
    tiles = seqs // LANES
    units = tiles * (prop // 2)
    others = max(tp // 2 - 1, 1)
    vmem, dma = pltpu.VMEM, pltpu.SemaphoreType.DMA
    return pl.pallas_call(
        functools.partial(step_kernel, kv, tp),
        in_specs=[pl.BlockSpec(memory_space=pl.ANY)] * len(args),
        out_specs=[pl.BlockSpec(memory_space=pltpu.VMEM)] * 2,
        out_shape=[vmem((prop, own, seqs), bf16), vmem(state.shape, f32)],
        scratch_shapes=[
            vmem((units, chips, 2, own, 2 * LANES), bf16),
            vmem((rows, width), bf16),
            vmem((width, 128), f32),
            vmem((2, width, cols), bf16),
            vmem(wo.shape, bf16),
            vmem((kv, 2, small, part), bf16),
            vmem((kv, part, 2 * small), bf16),
            vmem((prop, seqs, cols), bf16),
            vmem((prop, hd, LANES), f32),
            vmem((2, prop, seqs, cols), bf16),
            vmem((2, prop, cols, seqs), f32),
            vmem((prop, heads, 8, seqs), f32),
            vmem((2, prop, small, seqs), bf16),
            vmem((prop, small, seqs), f32),
            vmem((tiles, heads * prop, LANES), f32),
            vmem((tiles, tp, heads * prop, LANES), f32),
            vmem((units, kv, 2, small, 2 * LANES), bf16),
            vmem((units, part // own, own, 2 * LANES), f32),
            vmem((units, part // own, own, 2 * LANES), bf16),
            vmem((units, others, own, 2 * LANES), bf16),
            vmem((tiles, kv * tp, prop // 2, 2 * LANES), f32),
        ]
        + [vmem(x.shape, x.dtype) for x in args[7:]]
        + [
            dma((len(args) - 2,)),
            dma((units, 2)),
            dma((tiles, heads)),
            dma((units,)),
            dma((units, 2, chips)),
            dma((2, units)),
            dma((2,)),
            dma((kv,)),
            dma((tiles, tp)),
            dma((tiles, tp)),
            dma((units,)),
            dma((units, 1, kv)),
            dma((2, units)),
            dma((units, others)),
            dma((units, others)),
            dma((tiles,)),
            dma((tiles, kv * tp)),
        ],
        compiler_params=pltpu.CompilerParams(
            collective_id=0, has_side_effects=True, vmem_limit_bytes=VMEM_ALL - (9 << 20)
        ),
        cost_estimate=pl.CostEstimate(
            flops=2 * rows * width * prop * seqs, bytes_accessed=16 << 20, transcendentals=0
        ),
    )(*[x if x.size == 1 else pltpu.with_memory_space_constraint(x, pltpu.HBM) for x in args])


def on_device(
    kv,
    tp,
    tokens,
    input_norm_gain,
    query_weight,
    key_weight,
    value_weight,
    output_gate_weight,
    strength_weight,
    decay_weight,
    head_decay_rate,
    proposal_log_decay,
    head_norm_gain,
    output_weight,
    output_norm_gain,
    state,
    previous_keys,
    previous_values,
    previous_log_decay,
    previous_strengths,
    accepted,
    parent,
):
    seqs, heads, vdim, hd = state.shape
    prop = parent.shape[1]
    width = input_norm_gain.shape[0]
    channels = heads * vdim

    def turn(x):
        return jnp.transpose(x, (1, 2, 0))

    layer_out, accepted_state = step(
        kv, tp,
        turn(tokens),
        query_weight,
        key_weight,
        turn(value_weight).reshape(channels, width),
        turn(output_gate_weight).reshape(channels, width),
        output_weight.reshape(channels, width),
        state,
        input_norm_gain.reshape(width // 128, 128),
        strength_weight.T,
        decay_weight.T,
        head_decay_rate[None, :],
        turn(proposal_log_decay),
        turn(previous_strengths),
        turn(previous_log_decay),
        accepted[None, :],
        parent.T,
        previous_keys,
        jnp.transpose(previous_values, (1, 2, 3, 0)).reshape(prop, channels, seqs),
        head_norm_gain[None, :],
        output_norm_gain[None, :],
    )
    return (jnp.transpose(layer_out, (2, 0, 1)), accepted_state)


def solution(mesh):
    placed = (
        P(None, None, AXES),
        P(),
        P(None, "kv"),
        P(None, "kv"),
        P(None, "kv", "tp"),
        P(None, "kv", "tp"),
        P(None, "kv"),
        P(None, "kv"),
        P("kv"),
        P(None, None, "kv"),
        P("tp"),
        P("kv", "tp", None),
        P(AXES),
        P(None, "kv", "tp", None),
        P(None, None, "kv"),
        P(None, None, "kv", "tp"),
        P(None, None, "kv"),
        P(None, None, "kv"),
        P(),
        P(),
    )
    return jax.shard_map(
        functools.partial(on_device, mesh.shape["kv"], mesh.shape["tp"]),
        mesh=mesh,
        in_specs=placed,
        out_specs=(P(None, None, AXES), P(None, "kv", "tp", None)),
        check_vma=False,
    )
```
